128 devices in a mesh: sp: 16 (over z, y), dp: 8 (over x, core).
Axes of the slice: x: 4, y: 4, z: 4, core: 2. Of those that a mesh axis runs over, the one named last changes fastest.
Arguments:
- query_nope: bfloat16 [8, 4096, 16, 128], P('dp', 'sp'), may hold values from -6 to 6
- query_rope: bfloat16 [8, 4096, 16, 64], P('dp', 'sp'), may hold values from -160 to 160
- latent: bfloat16 [8, 4096, 256], P('dp', 'sp'), may hold values from -6 to 6
- key_rope: bfloat16 [8, 4096, 64], P('dp', 'sp'), may hold values from -4 to 4
- resid: bfloat16 [8, 4096, 2048], P('dp', 'sp'), may hold values from -6 to 6
- latent_gain: float32 [256], replicated, may hold values from 0.1 to 1.9
- key_up: bfloat16 [256, 2048], P(None, 'sp'), may hold values from -0.375 to 0.375
- value_up: bfloat16 [256, 2048], P(None, 'sp'), may hold values from -0.375 to 0.375
- out_proj: bfloat16 [2048, 2048], P('sp', 'dp'), may hold values from -0.125 to 0.125
- norm_gain: float32 [2048], replicated, may hold values from 0.1 to 1.9
- expert_gate: bfloat16 [16, 2048, 1024], P('sp'), may hold values from -0.125 to 0.125
- expert_up: bfloat16 [16, 2048, 1024], P('sp'), may hold values from -0.125 to 0.125
- expert_down: bfloat16 [16, 1024, 2048], P('sp'), may hold values from -0.1875 to 0.1875
- routes: int32 [8, 4096, 2], P('dp', 'sp'), may hold values from 0 to 15, all different within a row; in each aligned block of 256 rows (0 to 255, 256 to 511, ..., all dimensions but the last counted through in order) at most 64 rows name the same one
- route_weight: float32 [8, 4096, 2], P('dp', 'sp'), may hold values from 0.2 to 1
Outputs:
- mixed: bfloat16 [8, 4096, 2048], P('dp', 'sp')
The draws below stay inside these ranges and needn't reach their ends.
Inputs may be any that keep to these rules, and one draw needn't show every extreme that they name: `routes`: each token names two different experts. Among the tokens of one device no expert is named more than 64 times, and in every draw some expert is named exactly 64 times by some device's tokens.
All inputs are finite; a program needn't handle non-finite values.
Results may differ from the reference program's by a relative error of at most 0.0075.
Values may be sent and summed in bfloat16 or wider, within the bound.
A program may use at most 128 MiB of HBM per device.

```python
import math
import jax
import jax.numpy as jnp
import numpy as np
from jax import lax

D = 2048
HEADS = 16
NOPE = 128
ROPE = 64
VDIM = 128
LATENT = 256
FFE = 1024
TOK_DEV = 256
LENGTH = 4096
SEQS = 8
EXPERTS = 16
CAP = 64
N_SP = 16
N_DP = 8


def rope_pair(key):
    base_key = jax.random.fold_in(key, 911)
    key_draw, query_draw = jax.random.split(base_key, 2)
    keys_raw = jnp.clip(jax.random.normal(key_draw, (SEQS, LENGTH, ROPE), jnp.float32), -4.0, 4.0)
    queries = jnp.clip(jax.random.normal(query_draw, (SEQS, LENGTH, HEADS, ROPE), jnp.float32), -4.0, 4.0)
    return (queries, keys_raw)


def draw_query_rope(key, part):
    return rope_pair(key)[0].astype(jnp.bfloat16)


def draw_key_rope(key, part):
    return rope_pair(key)[1].astype(jnp.bfloat16)


def steps_of(rng, extent, cuts, low, top_value):
    def one(axis_at, parts):
        steps = jax.random.uniform(jax.random.fold_in(jax.random.fold_in(rng, 6), axis_at), (parts,), jnp.float32, low / len(cuts), top_value / len(cuts))
        return jnp.repeat(jnp.exp(steps), extent[axis_at] // parts).reshape((-1,) + (1,) * (len(extent) - axis_at - 1))

    factor_of = one(*cuts[0])
    for cut in cuts[1:]:
        factor_of = factor_of * one(*cut)
    return factor_of


def deal_out(key, own, number, rows, count, top, most, lean):
    order = jax.random.permutation(key, count)
    heavy_load, usual = load_shares(count, rows * top, most, lean, True), load_shares(count, rows * top, most, lean, False)
    places = jnp.arange(count)

    def named(tallies, offset_by):
        used = int((tallies > 0).sum())
        fixed = max(1, used // 4)
        shifted = fixed + (places - fixed + offset_by * (used - fixed)) % max(1, count - fixed)
        return jnp.zeros((count,), jnp.int32).at[order[jnp.where(places < fixed, places, shifted)]].set(jnp.asarray(tallies, jnp.int32))

    tallies = jnp.where(number % 4 == 0, named(heavy_load, number // 4), named(usual, number - number // 4 - 1))
    mixed = jax.random.permutation(jax.random.fold_in(own, 3), count)
    giver, receiver = mixed[0:count // 2 * 2:2], mixed[1:count // 2 * 2:2]
    slack = jnp.minimum(tallies[giver] - 1, most - tallies[receiver]) // 2
    slack = jnp.where((giver == order[0]) | (receiver == order[0]) | (tallies[receiver] == 0), 0, jnp.maximum(slack, 0))
    shifted = jax.random.randint(jax.random.fold_in(own, 4), (count // 2,), 0, 1 << 20) % (slack + 1)
    tallies = tallies.at[giver].add(-shifted).at[receiver].add(shifted)
    items = jnp.searchsorted(jnp.cumsum(tallies), jnp.arange(rows * top), side="right").astype(jnp.int32)
    listing = items.reshape(top, rows).T
    listing = listing[jax.random.permutation(jax.random.fold_in(own, 1), rows)]
    offset_by = jax.random.randint(jax.random.fold_in(own, 2), (rows, 1), 0, top)
    return jnp.take_along_axis(listing, (jnp.arange(top)[None, :] + offset_by) % top, axis=1)


def load_shares(number_of, total, limit, slope, full):
    portions = [(1 << 20) // math.isqrt(standing ** slope) + 1 for standing in range(1, number_of + 1)]
    largest = limit if full else min(limit, max(-(-total // number_of), total * portions[0] // sum(portions)))
    least = 1 if total - largest >= number_of - 1 else 0
    counts, rest = [largest] + [least] * (number_of - 1), total - largest - least * (number_of - 1)
    while rest > 0:
        candidates = [i for i in range(1, number_of) if counts[i] < largest] or [i for i in range(1, number_of) if counts[i] < limit]
        mass, remaining = sum([portions[i] for i in candidates]), rest
        for i in candidates:
            more = min(limit - counts[i], max(1, remaining * portions[i] // mass), rest)
            counts[i] = counts[i] + more
            rest = rest - more
    return np.array(counts)


def centred(key, shape, deviation, reach, cuts=(), held_as=jnp.bfloat16):
    drawn = jax.random.normal(key, shape, jnp.float32) * deviation
    if len(cuts) > 0:
        drawn = steps_of(key, shape, cuts, -0.22, 0.18) * drawn
    return jnp.clip(drawn, min=-reach, max=reach).astype(held_as)


def setup_inputs(seed: int = 0) -> dict:
    keys = jax.random.split(jax.random.key(seed), 16)
    query_nope = centred(keys[0], (SEQS, LENGTH, HEADS, NOPE), 1.0, 6.0, ((0, 8), (1, 16)))
    query_rope = draw_query_rope(jax.random.fold_in(keys[15], 71), 0)
    latent = centred(keys[2], (SEQS, LENGTH, LATENT), 1.0, 6.0, ((0, 8), (1, 16)))
    key_rope = draw_key_rope(jax.random.fold_in(keys[15], 71), 0)
    resid = centred(keys[4], (SEQS, LENGTH, D), 1.0, 6.0, ((0, 8), (1, 16)))
    latent_gain = jnp.clip(1.0 + 0.18 * jax.random.normal(keys[5], (LATENT,), jnp.float32), 0.1, 1.9)
    key_up = centred(keys[6], (LATENT, HEADS * NOPE), LATENT ** -0.5, 0.375, ((1, 16),))
    value_up = centred(keys[7], (LATENT, HEADS * VDIM), LATENT ** -0.5, 0.375, ((1, 16),))
    out_proj = centred(keys[8], (HEADS * VDIM, D), (HEADS * VDIM) ** -0.5, 0.125, ((0, 16), (1, 8)))
    norm_gain = jnp.clip(1.0 + 0.18 * jax.random.normal(keys[9], (D,), jnp.float32), 0.1, 1.9)
    expert_gate = centred(keys[10], (EXPERTS, D, FFE), D ** -0.5, 0.125, ((0, 16),))
    expert_up = centred(keys[11], (EXPERTS, D, FFE), D ** -0.5, 0.125, ((0, 16),))
    expert_down = centred(keys[12], (EXPERTS, FFE, D), FFE ** -0.5, 0.1875, ((0, 16),))
    routes_keys = jax.random.split(jax.random.fold_in(keys[13], 1), SEQS * LENGTH // TOK_DEV)
    routes_turns = jax.random.permutation(jax.random.fold_in(keys[13], 3), SEQS * LENGTH // TOK_DEV)
    routes = jax.vmap(lambda own, number: deal_out(jax.random.fold_in(keys[13], 2), own, number, TOK_DEV, EXPERTS, 2, CAP, 1))(routes_keys, routes_turns).reshape((SEQS, LENGTH, 2))
    route_weight = jnp.clip(0.2 + 0.8 * jax.random.uniform(keys[14], (SEQS, LENGTH, 2), jnp.float32) ** steps_of(keys[14], (SEQS, LENGTH, 2), ((0, 8), (1, 16)), -0.2, 0.2), 0.2, 1.0)
    return dict(query_nope=query_nope, query_rope=query_rope, latent=latent, key_rope=key_rope, resid=resid, latent_gain=latent_gain, key_up=key_up, value_up=value_up, out_proj=out_proj, norm_gain=norm_gain, expert_gate=expert_gate, expert_up=expert_up, expert_down=expert_down, routes=routes, route_weight=route_weight)


epsilon = 1e-06
rope_base = 10000.0
masked_score = -1e+30

def rotate(values, positions):
    half_width = values.shape[-1] // 2
    frequency = rope_base ** (-jnp.arange(half_width, dtype=jnp.float32) / half_width)
    angles = positions.astype(jnp.float32)[:, None] * frequency[None, :]
    cosine = jnp.cos(angles)
    sine_part = jnp.sin(angles)
    if values.ndim == 3:
        cosine = cosine[:, None, :]
        sine_part = sine_part[:, None, :]
    floats = values.astype(jnp.float32)
    first_half = floats[..., :half_width]
    second_half = floats[..., half_width:]
    turned = jnp.concatenate([first_half * cosine - second_half * sine_part, second_half * cosine + first_half * sine_part], axis=-1)
    return turned.astype(jnp.bfloat16)

def rms_scaled(values, gain):
    floats = values.astype(jnp.float32)
    return floats * lax.rsqrt(lax.optimization_barrier(jnp.mean(floats * floats, axis=-1, keepdims=True)) + epsilon) * gain

def assign_slots(route_block, experts_all, capacity):
    flat_routes = route_block.reshape(-1)
    onehot = (flat_routes[:, None] == jnp.arange(experts_all, dtype=jnp.int32)[None, :]).astype(jnp.int32)
    earlier = jnp.cumsum(onehot, axis=0) - onehot
    placed = lax.optimization_barrier(jnp.sum(earlier * onehot, axis=1))
    return (flat_routes * capacity + placed).astype(jnp.int32)

def fill_slots(rows, slot_ids, experts_all, capacity):
    pairs = slot_ids.shape[0]
    matches = jnp.arange(experts_all * capacity, dtype=jnp.int32)[:, None] == slot_ids[None, :]
    source = lax.optimization_barrier(jnp.sum(jnp.where(matches, jnp.arange(pairs, dtype=jnp.int32)[None, :], 0), axis=1)) // 2
    filled = jnp.any(matches, axis=1)
    picked = jnp.take(rows, source.astype(jnp.int32), axis=0)
    chosen = jnp.where(filled[:, None], picked, jnp.zeros_like(picked))
    return chosen.reshape(experts_all, capacity, rows.shape[-1])

def combine_slots(returned, slot_ids, weights):
    flat_back = returned.reshape(-1, returned.shape[-1])
    picked = jnp.take(flat_back, slot_ids, axis=0).astype(jnp.float32).reshape(weights.shape[0], 2, -1)
    return lax.optimization_barrier(jnp.sum(weights[:, :, None] * picked, axis=1))

def expert_rows(rows, gate_weight, up_weight, down_weight):
    gate = jnp.dot(rows, gate_weight, preferred_element_type=jnp.float32)
    upward = jnp.dot(rows, up_weight, preferred_element_type=jnp.float32)
    hidden = (jax.nn.silu(gate) * upward).astype(jnp.bfloat16)
    return jnp.dot(hidden, down_weight, preferred_element_type=jnp.float32).astype(jnp.bfloat16)

def head_attention(query_plain, query_turn, key_plain, key_turn, value_head, block):
    length = key_plain.shape[0]
    blocks = length // block
    scale = (query_plain.shape[-1] + query_turn.shape[-1]) ** (-0.5)
    key_ids = jnp.arange(length, dtype=jnp.int32)

    def one_block(items):
        index, plain_block, turn_block = items
        scores = jnp.dot(plain_block, key_plain.T, preferred_element_type=jnp.float32)
        scores = (scores + jnp.dot(turn_block, key_turn.T, preferred_element_type=jnp.float32)) * scale
        row_ids = index * block + jnp.arange(block, dtype=jnp.int32)
        allowed = key_ids[None, :] <= row_ids[:, None]
        scores = jnp.where(allowed, scores, masked_score)
        largest = lax.optimization_barrier(jnp.max(scores, axis=-1, keepdims=True))
        powers = jnp.exp(scores - largest)
        attend = (powers / lax.optimization_barrier(jnp.sum(powers, axis=-1, keepdims=True))).astype(jnp.bfloat16)
        return jnp.dot(attend, value_head, preferred_element_type=jnp.float32).astype(jnp.bfloat16)
    result = lax.map(one_block, (jnp.arange(blocks, dtype=jnp.int32), query_plain.reshape(blocks, block, -1), query_turn.reshape(blocks, block, -1)))
    return result.reshape(length, -1)

def reference(query_nope, query_rope, latent, key_rope, resid, latent_gain, key_up, value_up, out_proj, norm_gain, expert_gate, expert_up, expert_down, routes, route_weight):
    positions = jnp.arange(LENGTH, dtype=jnp.int32)
    block = min(512, LENGTH)
    key_turned = jax.vmap(lambda item: rotate(item, positions))(key_rope)
    query_turned = jax.vmap(lambda item: rotate(item, positions))(query_rope)
    latent_normed = rms_scaled(latent, latent_gain).astype(jnp.bfloat16)
    flat_latent = latent_normed.reshape(-1, LATENT)
    key_nope = jnp.dot(flat_latent, key_up, preferred_element_type=jnp.float32).astype(jnp.bfloat16).reshape(SEQS, LENGTH, HEADS, NOPE)
    values = jnp.dot(flat_latent, value_up, preferred_element_type=jnp.float32).astype(jnp.bfloat16).reshape(SEQS, LENGTH, HEADS, VDIM)

    def one_sequence(items):
        plain_heads, turn_heads, key_heads, value_heads, key_turn = items
        return lax.map(lambda head: head_attention(head[0], head[1], head[2], key_turn, head[3], block), (plain_heads, turn_heads, key_heads, value_heads))
    heads_out = lax.map(one_sequence, (jnp.transpose(query_nope, (0, 2, 1, 3)), jnp.transpose(query_turned, (0, 2, 1, 3)), jnp.transpose(key_nope, (0, 2, 1, 3)), jnp.transpose(values, (0, 2, 1, 3)), key_turned))
    heads_out = jnp.transpose(heads_out, (0, 2, 1, 3)).reshape(SEQS * LENGTH, HEADS * VDIM)
    projected = jnp.dot(heads_out, out_proj, preferred_element_type=jnp.float32).astype(jnp.bfloat16)
    after_attention = resid.reshape(-1, D).astype(jnp.float32) + projected.astype(jnp.float32)
    normed = rms_scaled(after_attention, norm_gain).astype(jnp.bfloat16)
    normed_blocks = normed.reshape(N_DP, N_SP, TOK_DEV, D)
    route_blocks = routes.reshape(N_DP, N_SP, TOK_DEV, 2)
    slot_ids = jax.vmap(jax.vmap(lambda item: assign_slots(item, EXPERTS, CAP)))(route_blocks)
    buffers = jax.vmap(jax.vmap(lambda rows, ids: fill_slots(rows, ids, EXPERTS, CAP)))(normed_blocks, slot_ids)
    by_expert = jnp.transpose(buffers, (2, 0, 1, 3, 4)).reshape(EXPERTS, N_DP * N_SP * CAP, D)
    outputs = lax.map(lambda item: expert_rows(item[0], item[1], item[2], item[3]), (by_expert, expert_gate, expert_up, expert_down))
    returned = jnp.transpose(outputs.reshape(EXPERTS, N_DP, N_SP, CAP, D), (1, 2, 0, 3, 4))
    routed = jax.vmap(jax.vmap(combine_slots))(returned, slot_ids, route_weight.reshape(N_DP, N_SP, TOK_DEV, 2))
    mixed = after_attention + routed.reshape(-1, D)
    return mixed.astype(jnp.bfloat16).reshape(SEQS, LENGTH, D)
```

```python
import jax
import jax.numpy as jnp
from jax import lax
from jax.experimental import pallas as pl
from jax.experimental.pallas import tpu as pltpu
from jax.sharding import PartitionSpec as P

epsilon = 1e-06
rope_base = 10000.0
masked_score = -1e30


def sent_together(arrays, axis, dim, along):
    both = jnp.concatenate(arrays, axis=along)
    out, at, finished = (lax.all_gather(both, axis, axis=dim, tiled=True), 0, [])
    for a in arrays:
        finished.append(lax.slice_in_dim(out, at, at + a.shape[along], axis=along))
        at += a.shape[along]
    return tuple(finished)


def rotate(values, positions):
    half_width = values.shape[-1] // 2
    frequency = rope_base ** (-jnp.arange(half_width, dtype=jnp.float32) / half_width)
    angles = positions.astype(jnp.float32)[:, None] * frequency[None, :]
    cosine = jnp.cos(angles)
    sine_part = jnp.sin(angles)
    if values.ndim == 3:
        cosine = cosine[:, None, :]
        sine_part = sine_part[:, None, :]
    floats = values.astype(jnp.float32)
    first_half = floats[..., :half_width]
    second_half = floats[..., half_width:]
    turned = jnp.concatenate(
        [
            first_half * cosine - second_half * sine_part,
            second_half * cosine + first_half * sine_part,
        ],
        axis=-1,
    )
    return turned.astype(jnp.bfloat16)


def rms_scaled(values, gain):
    floats = values.astype(jnp.float32)
    return floats * lax.rsqrt(jnp.mean(floats * floats, axis=-1, keepdims=True) + epsilon) * gain


ORDER = [(0, 0), (2, 2), (3, 2), (2, 3), (1, 2), (2, 1), (0, 2), (2, 0), (3, 1), (1, 3), (3, 3), (1, 1), (3, 0), (0, 3), (1, 0), (0, 1)]
MESH = pl.DeviceIdType.MESH


def shifted(me, dz, dy):
    z, y = me // 4, lax.rem(me, 4)
    return lax.rem(z + dz, 4) * 4 + lax.rem(y + dy, 4)


def remote(src, dst, send, recv, target):
    return pltpu.make_async_remote_copy(
        src_ref=src,
        dst_ref=dst,
        send_sem=send,
        recv_sem=recv,
        device_id={"sp": target},
        device_id_type=MESH,
    )


def experts_kernel(
    heads, wo, resid, gain, routes, routes_t, weight, wg_hbm, wu_hbm, wd_hbm, out,
    wg, wu, wd, after, normed, outgoing, arrived, hidden, result, returned, total,
    wsem, send1, recv1, send2, recv2,
):
    me = lax.axis_index("sp")
    f32, bf16, i32 = jnp.float32, jnp.bfloat16, jnp.int32
    barrier = pltpu.get_barrier_semaphore()
    for dz, dy in ORDER[1:]:
        pl.semaphore_signal(barrier, inc=1, device_id={"sp": shifted(me, dz, dy)}, device_id_type=MESH)
    loads = [
        pltpu.make_async_copy(a, b, wsem.at[i])
        for i, (a, b) in enumerate(((wg_hbm, wg), (wu_hbm, wu), (wd_hbm, wd)))
    ]
    for load in loads:
        load.start()

    @pl.loop(0, 8)
    def _(n):
        cols = pl.ds(pl.multiple_of(n * 256, 256), 256)
        p = jnp.dot(heads[...], wo[:, cols], preferred_element_type=f32).astype(bf16)
        after[:, cols] = resid[:, cols].astype(f32) + p.astype(f32)

    @pl.loop(0, 8)
    def _(r):
        rows = pl.ds(pl.multiple_of(r * 32, 32), 32)
        a = after[rows, :]
        scale = lax.rsqrt(jnp.mean(a * a, axis=-1, keepdims=True) + epsilon)
        normed[rows, :] = (a * scale * gain[...]).astype(bf16)

    tok = lax.broadcasted_iota(i32, (256, 256), 0)
    tok_l = lax.broadcasted_iota(i32, (256, 256), 1)
    upper = jnp.where(tok < tok_l, 1.0, 0.0).astype(bf16)
    lower = jnp.where(tok_l < tok, 1.0, 0.0).astype(bf16)
    ex_t = lax.broadcasted_iota(i32, (16, 256), 0)
    hot_t = [jnp.where(ex_t == routes_t[k : k + 1, :], 1.0, 0.0) for k in range(2)]
    before_t = jnp.dot((hot_t[0] + hot_t[1]).astype(bf16), upper, preferred_element_type=f32)
    base_t = before_t + (ex_t * 64).astype(f32)
    slot_t = [jnp.sum(h * base_t, axis=0, keepdims=True).astype(i32) for h in hot_t]
    ex_c = lax.broadcasted_iota(i32, (256, 128), 1)
    hot_c = [jnp.where(ex_c == routes[:, k : k + 1], 1.0, 0.0) for k in range(2)]
    before_c = jnp.dot(lower, (hot_c[0] + hot_c[1]).astype(bf16), preferred_element_type=f32)
    base_c = before_c + (ex_c * 64).astype(f32)
    slot_c = [jnp.sum(h * base_c, axis=1, keepdims=True).astype(i32) for h in hot_c]

    def places(g, axis):
        shape = (256, 1) if axis == 0 else (1, 256)
        r = lax.broadcasted_iota(i32, shape, axis)
        owner = [shifted(me, *ORDER[4 * g + j]) * 64 for j in range(4)]
        base = jnp.where(r < 64, owner[0], jnp.where(r < 128, owner[1], jnp.where(r < 192, owner[2], owner[3])))
        return base + (r & 63)

    pl.semaphore_wait(barrier, 15)

    first = [
        None if k == 0 else remote(outgoing.at[k], arrived.at[k], send1.at[k], recv1.at[k], shifted(me, *ORDER[k]))
        for k in range(16)
    ]
    for g in range(4):
        place = places(g, 0)
        pick = jnp.where((slot_t[0] == place) | (slot_t[1] == place), 1.0, 0.0).astype(bf16)
        for n in range(4):
            cols = slice(n * 512, n * 512 + 512)
            rows = jnp.dot(pick, normed[:, cols], preferred_element_type=f32).astype(bf16)
            for j in range(4):
                k = 4 * g + j
                (arrived if k == 0 else outgoing)[k, :, cols] = rows[j * 64 : j * 64 + 64]
        if g > 0:
            for k in range(max(1, 4 * g - 4), 4 * g):
                first[k].start()
    for load in loads:
        load.wait()
    for k in range(12, 16):
        first[k].start()

    second = [
        None if k == 0 else remote(result.at[k], returned.at[k], send2.at[k], recv2.at[k], shifted(me, (4 - ORDER[k][0]) % 4, (4 - ORDER[k][1]) % 4))
        for k in range(16)
    ]
    for g in range(4):
        for k in range(max(1, 4 * g), 4 * g + 4):
            first[k].wait_recv()

        @pl.loop(0, 4)
        def _(n):
            cols = pl.ds(pl.multiple_of(n * 256, 256), 256)
            rows = arrived[4 * g : 4 * g + 4].reshape(256, 2048)
            gate = jnp.dot(rows, wg[:, cols], preferred_element_type=f32)
            up = jnp.dot(rows, wu[:, cols], preferred_element_type=f32)
            hidden[:, cols] = (gate / (1.0 + jnp.exp(-gate)) * up).astype(bf16)

        @pl.loop(0, 4)
        def _(n):
            cols = pl.ds(pl.multiple_of(n * 512, 512), 512)
            rows = jnp.dot(hidden[...], wd[:, cols], preferred_element_type=f32).astype(bf16)
            for j in range(4):
                k = 4 * g + j
                (returned if k == 0 else result)[k, :, cols] = rows[j * 64 : j * 64 + 64]

        for k in range(max(1, 4 * g), 4 * g + 4):
            second[k].start()

    for g in range(4):
        place = places(g, 1)
        picks = [jnp.where(s == place, 1.0, 0.0).astype(bf16) for s in slot_c]
        for k in range(max(1, 4 * g), 4 * g + 4):
            second[k].wait_recv()
        for n in range(4):
            cols = slice(n * 512, n * 512 + 512)
            rows = returned[4 * g : 4 * g + 4, :, cols].reshape(256, 512)
            t = weight[:, 0:1] * jnp.dot(picks[0], rows, preferred_element_type=f32)
            t = t + weight[:, 1:2] * jnp.dot(picks[1], rows, preferred_element_type=f32)
            if g > 0:
                t = t + total[:, cols]
            if g < 3:
                total[:, cols] = t
            else:
                out[:, cols] = (after[:, cols] + t).astype(bf16)
    for k in range(1, 16):
        first[k].wait_send()
        second[k].wait_send()


def experts(heads, wo, resid, gain, routes, weight, wg, wu, wd):
    v, a = pl.BlockSpec(memory_space=pltpu.VMEM), pl.BlockSpec(memory_space=pl.ANY)
    bf16, f32 = jnp.bfloat16, jnp.float32
    return pl.pallas_call(
        experts_kernel,
        name="experts",
        out_shape=jax.ShapeDtypeStruct((256, 2048), bf16),
        in_specs=[v] * 7 + [a] * 3,
        out_specs=v,
        scratch_shapes=[
            pltpu.VMEM((2048, 1024), bf16),
            pltpu.VMEM((2048, 1024), bf16),
            pltpu.VMEM((1024, 2048), bf16),
            pltpu.VMEM((256, 2048), f32),
            pltpu.VMEM((256, 2048), bf16),
            pltpu.VMEM((16, 64, 2048), bf16),
            pltpu.VMEM((16, 64, 2048), bf16),
            pltpu.VMEM((256, 1024), bf16),
            pltpu.VMEM((16, 64, 2048), bf16),
            pltpu.VMEM((16, 64, 2048), bf16),
            pltpu.VMEM((256, 2048), f32),
            pltpu.SemaphoreType.DMA((3,)),
        ]
        + [pltpu.SemaphoreType.DMA((16,))] * 4,
        compiler_params=pltpu.CompilerParams(
            collective_id=1, has_side_effects=True, vmem_limit_bytes=60 * 1024 * 1024
        ),
    )(heads, wo, resid, gain, routes, routes.T, weight, wg, wu, wd)


def shards(
    query_nope,
    query_rope,
    latent,
    key_rope,
    resid,
    latent_gain,
    key_up,
    value_up,
    out_proj,
    norm_gain,
    expert_gate,
    expert_up,
    expert_down,
    routes,
    route_weight,
):
    tokens_here = latent.shape[1]
    sp_count = lax.axis_size("sp")
    length = tokens_here * sp_count
    block = min(512, length)
    blocks = length // block
    local_pos = lax.axis_index("sp") * tokens_here + jnp.arange(tokens_here, dtype=jnp.int32)
    latent_normed = rms_scaled(latent[0], latent_gain).astype(jnp.bfloat16)
    key_turned = rotate(key_rope[0], local_pos)
    query_turned = rotate(query_rope[0], local_pos)
    all_latent, all_keyturn = sent_together((latent_normed, key_turned), "sp", 0, 1)
    query_plain, query_turn = (
        lax.all_to_all(query_nope[0], "sp", split_axis=1, concat_axis=0, tiled=True),
        lax.all_to_all(query_turned, "sp", split_axis=1, concat_axis=0, tiled=True),
    )
    heads_here = query_plain.shape[1]
    key_plain = (
        jnp.dot(all_latent, key_up, preferred_element_type=jnp.float32)
        .astype(jnp.bfloat16)
        .reshape(length, heads_here, -1)
    )
    value_heads = (
        jnp.dot(all_latent, value_up, preferred_element_type=jnp.float32)
        .astype(jnp.bfloat16)
        .reshape(length, heads_here, -1)
    )
    scale = (query_plain.shape[-1] + query_turn.shape[-1]) ** (-0.5)
    key_ids = jnp.arange(length, dtype=jnp.int32)

    def one_block(items):
        index, plain_block, turn_block = items
        scores = jnp.einsum(
            "bhd,shd->hbs", plain_block, key_plain, preferred_element_type=jnp.float32
        )
        scores = (
            scores
            + jnp.einsum("bhr,sr->hbs", turn_block, all_keyturn, preferred_element_type=jnp.float32)
        ) * scale
        row_ids = index * block + jnp.arange(block, dtype=jnp.int32)
        allowed = key_ids[None, :] <= row_ids[:, None]
        scores = jnp.where(allowed[None], scores, masked_score)
        largest = jnp.max(scores, axis=-1, keepdims=True)
        powers = jnp.exp(scores - largest)
        attend = (powers / jnp.sum(powers, axis=-1, keepdims=True)).astype(jnp.bfloat16)
        return jnp.einsum(
            "hbs,shd->bhd", attend, value_heads, preferred_element_type=jnp.float32
        ).astype(jnp.bfloat16)

    attended = lax.map(
        one_block,
        (
            jnp.arange(blocks, dtype=jnp.int32),
            query_plain.reshape(blocks, block, heads_here, -1),
            query_turn.reshape(blocks, block, heads_here, -1),
        ),
    )
    attended = attended.reshape(length, heads_here, -1)
    token_heads = lax.all_to_all(attended, "sp", split_axis=0, concat_axis=1, tiled=True)
    flat_heads = token_heads.reshape(tokens_here, -1)
    head_rows = lax.all_gather(out_proj, "dp", axis=1, tiled=True)
    wo = lax.all_gather(head_rows, "sp", axis=0, tiled=True)
    return experts(
        flat_heads, wo, resid[0], norm_gain[None], routes[0], route_weight[0],
        expert_gate[0], expert_up[0], expert_down[0],
    )[None]


def solution(mesh):
    return jax.shard_map(
        shards,
        mesh=mesh,
        in_specs=(
            P("dp", "sp", None, None),
            P("dp", "sp", None, None),
            P("dp", "sp", None),
            P("dp", "sp", None),
            P("dp", "sp", None),
            P(),
            P(None, "sp"),
            P(None, "sp"),
            P("sp", "dp"),
            P(),
            P("sp", None, None),
            P("sp", None, None),
            P("sp", None, None),
            P("dp", "sp", None),
            P("dp", "sp", None),
        ),
        out_specs=P("dp", "sp", None),
        check_vma=False,
    )
```

```python
import jax
import jax.numpy as jnp
from jax import lax
from jax.experimental import pallas as pl
from jax.experimental.pallas import tpu as pltpu
from jax.sharding import PartitionSpec as P

epsilon = 1e-06
rope_base = 10000.0
masked_score = -1e30


def rotate(values, positions):
    half_width = values.shape[-1] // 2
    frequency = rope_base ** (-jnp.arange(half_width, dtype=jnp.float32) / half_width)
    angles = positions.astype(jnp.float32)[:, None] * frequency[None, :]
    cosine = jnp.cos(angles)
    sine_part = jnp.sin(angles)
    if values.ndim == 3:
        cosine = cosine[:, None, :]
        sine_part = sine_part[:, None, :]
    floats = values.astype(jnp.float32)
    first_half = floats[..., :half_width]
    second_half = floats[..., half_width:]
    turned = jnp.concatenate(
        [
            first_half * cosine - second_half * sine_part,
            second_half * cosine + first_half * sine_part,
        ],
        axis=-1,
    )
    return turned.astype(jnp.bfloat16)


def rms_scaled(values, gain):
    floats = values.astype(jnp.float32)
    return floats * lax.rsqrt(jnp.mean(floats * floats, axis=-1, keepdims=True) + epsilon) * gain


ORDER = [(0, 0), (2, 2), (3, 2), (2, 3), (1, 2), (2, 1), (0, 2), (2, 0), (3, 1), (1, 3), (3, 3), (1, 1), (3, 0), (0, 3), (1, 0), (0, 1)]
MESH = pl.DeviceIdType.MESH


def packed(digits):
    value = sum(d << (2 * i) for i, d in enumerate(digits))
    return value - (1 << 32) if value >= 1 << 31 else value


ZS, YS = packed([o[0] for o in ORDER]), packed([o[1] for o in ORDER])


def shifted(me, dz, dy):
    z, y = me // 4, lax.rem(me, 4)
    return lax.rem(z + dz, 4) * 4 + lax.rem(y + dy, 4)


def remote(src, dst, send, recv, target):
    return pltpu.make_async_remote_copy(
        src_ref=src,
        dst_ref=dst,
        send_sem=send,
        recv_sem=recv,
        device_id={"sp": target},
        device_id_type=MESH,
    )


def layer_kernel(
    q_in_hbm, lat_a, lat_b, up_kv, wo_hbm, resid, gain, routes, routes_t, weight, wg_hbm, wu_hbm, wd_hbm, out,
    wg, wu, wd, after, normed, outgoing, arrived, hidden, result, returned, total,
    q_in, la, lb, keys, vals, q_cat, attended, heads, wo,
    wsem, send1, recv1, send2, recv2,
    lsem, sa1, ra1, sb1, rb1, sa2, ra2, sb2, rb2, sq, rq, so, ro, swz, rwz, swy, rwy, swx, rwx, swc, rwc,
):
    me, dp = lax.axis_index("sp"), lax.axis_index("dp")
    z, y = me // 4, lax.rem(me, 4)
    x, core = dp // 2, lax.rem(dp, 2)
    f32, bf16, i32 = jnp.float32, jnp.bfloat16, jnp.int32
    barrier = pltpu.get_barrier_semaphore()
    for dz, dy in ORDER[1:]:
        pl.semaphore_signal(barrier, inc=1, device_id={"sp": shifted(me, dz, dy)}, device_id_type=MESH)
    x_peer = [None] + [lax.rem(x + d, 4) * 2 + core for d in (1, 2, 3)]
    x_from = [dp] + [lax.rem(x + 4 - d, 4) * 2 + core for d in (1, 2, 3)]
    other = x * 2 + 1 - core
    for t in x_peer[1:] + [other]:
        pl.semaphore_signal(barrier, inc=1, device_id={"dp": t}, device_id_type=MESH)
    fill_wo = pltpu.make_async_copy(wo_hbm, wo.at[dp, z, y], lsem.at[0])
    fill_wo.start()
    fill_q = pltpu.make_async_copy(q_in_hbm.at[me], q_in.at[0], lsem.at[1])
    fill_q.start()
    fill_a = pltpu.make_async_copy(lat_a, la.at[z, y], lsem.at[2])
    fill_a.start()
    fill_b = pltpu.make_async_copy(lat_b, lb.at[z, y], lsem.at[3])
    fill_b.start()
    loads = [
        pltpu.make_async_copy(a, b, wsem.at[i])
        for i, (a, b) in enumerate(((wg_hbm, wg), (wu_hbm, wu), (wd_hbm, wd)))
    ]
    for load in loads:
        load.start()
    fill_a.wait()
    fill_b.wait()
    fill_wo.wait()
    pl.semaphore_wait(barrier, 19)

    def along(dz, dy):
        return shifted(me, dz, dy)

    a1 = [remote(la.at[z, y], la.at[z, y], sa1.at[d], ra1.at[d], along(d, 0)) for d in (1, 2, 3)]
    b1 = [remote(lb.at[z, y], lb.at[z, y], sb1.at[d], rb1.at[d], along(0, d)) for d in (1, 2, 3)]
    w1 = [remote(wo.at[dp, z, y], wo.at[dp, z, y], swz.at[d], rwz.at[d], along(d, 0)) for d in (1, 2, 3)]
    a2 = [remote(la.at[:, y], la.at[:, y], sa2.at[d], ra2.at[d], along(0, d)) for d in (1, 2, 3)]
    b2 = [remote(lb.at[z], lb.at[z], sb2.at[d], rb2.at[d], along(d, 0)) for d in (1, 2, 3)]
    w2 = [remote(wo.at[dp, :, y], wo.at[dp, :, y], swy.at[d], rwy.at[d], along(0, d)) for d in (1, 2, 3)]
    asks = [
        None if k == 0 else remote(q_in_hbm.at[along(*ORDER[k])], q_in.at[k], sq.at[k], rq.at[k], along(*ORDER[k]))
        for k in range(16)
    ]

    def to_x(g):
        part = wo.at[dp, :, lax.rem(y + 4 - g, 4)]
        copies = [
            pltpu.make_async_remote_copy(
                src_ref=part, dst_ref=part, send_sem=swx.at[g, d], recv_sem=rwx.at[g, d],
                device_id={"dp": x_peer[d]}, device_id_type=MESH,
            )
            for d in (1, 2, 3)
        ]
        return copies

    def to_core(g, d):
        part = wo.at[x_from[d], :, lax.rem(y + 4 - g, 4)]
        return pltpu.make_async_remote_copy(
            src_ref=part, dst_ref=part, send_sem=swc.at[g, d], recv_sem=rwc.at[g, d],
            device_id={"dp": other}, device_id_type=MESH,
        )

    for c in a1 + b1 + w1:
        c.start()
    for c in a1:
        c.wait_recv()
    for c in a2:
        c.start()
    for c in b1:
        c.wait_recv()
    for c in b2:
        c.start()
    for c in w1:
        c.wait_recv()
    for c in w2 + to_x(0) + [to_core(0, 0)]:
        c.start()
    for c in asks[1:]:
        c.start()

    vals[:, 128:256] = jnp.ones((4096, 128), bf16)
    for c in a2 + b2:
        c.wait_recv()

    @pl.loop(0, 16)
    def _(b):
        bz, by = b // 4, lax.rem(b, 4)
        rows = pl.ds(pl.multiple_of(b * 256, 256), 256)
        lat = jnp.concatenate([la[bz, by], lb[bz, by, 0:256, :]], axis=1)
        kv = jnp.dot(lat, up_kv[...], preferred_element_type=f32).astype(bf16)
        keys[rows, 0:128] = kv[:, 0:128]
        vals[rows, 0:128] = kv[:, 128:256]
        turn = lb[bz, by, 256:384, :].astype(f32)
        swap = pltpu.roll(turn, 64, 1)
        low = lax.broadcasted_iota(i32, (128, 128), 1) < 64
        start = pl.multiple_of(b * 256, 256)
        keys[pl.ds(start, 128), 128:256] = jnp.where(low, turn, swap).astype(bf16)
        keys[pl.ds(pl.multiple_of(start + 128, 128), 128), 128:256] = jnp.where(low, swap, turn).astype(bf16)

    fill_q.wait()
    unit = 192.0 ** -0.5

    def one_block(k, _):
        dz, dy = (ZS >> (2 * k)) & 3, (YS >> (2 * k)) & 3
        source = shifted(me, 4 - dz, 4 - dy)

        @pl.when(k > 0)
        def _():
            remote(q_in.at[k], q_in.at[k], sq.at[k], rq.at[k], source).wait_recv()

        for g in (1, 2, 3):

            @pl.when(k == 4 * g - 2)
            def _(g=g):
                w2[g - 1].wait_recv()
                for c in to_x(g) + [to_core(g, 0)]:
                    c.start()

        for g in (0, 1, 2):

            @pl.when(k == 5 * g + 5)
            def _(g=g):
                for d in (1, 2, 3):
                    to_x(g)[d - 1].wait_recv()
                    to_core(g, d).start()

        q_cat[:, 0:128] = q_in[k, 0:256, :]
        turn = q_in[k, 256:384, :]
        low = lax.broadcasted_iota(i32, (128, 128), 1) < 64
        zero = jnp.zeros((128, 128), bf16)
        q_cat[0:128, 128:256] = jnp.where(low, turn, zero)
        q_cat[128:256, 128:256] = jnp.where(low, zero, turn)
        q = q_cat[...]

        def scores(at):
            return lax.dot_general(
                q, keys[pl.ds(at, 512), :], (((1,), (1,)), ((), ())), preferred_element_type=f32
            ) * unit

        last = pl.multiple_of((source // 2) * 512, 512)
        s = scores(last)
        row_id = source * 256 + lax.broadcasted_iota(i32, (256, 512), 0)
        key_id = last + lax.broadcasted_iota(i32, (256, 512), 1)
        s = jnp.where(key_id <= row_id, s, masked_score)
        top = jnp.max(s, axis=-1, keepdims=True)
        p = jnp.exp(s - top).astype(bf16)
        acc = jnp.dot(p, vals[pl.ds(last, 512), :], preferred_element_type=f32)

        def step(i, carry):
            top, acc = carry
            at = pl.multiple_of(i * 512, 512)
            s = scores(at)
            new = jnp.maximum(top, jnp.max(s, axis=-1, keepdims=True))
            p = jnp.exp(s - new).astype(bf16)
            acc = acc * jnp.exp(top - new) + jnp.dot(p, vals[pl.ds(at, 512), :], preferred_element_type=f32)
            return new, acc

        top, acc = lax.fori_loop(0, source // 2, step, (top, acc))
        attended[k] = (acc[:, 0:128] / acc[:, 128:256]).astype(bf16)
        mine = pl.ds(pl.multiple_of(me * 128, 128), 128)

        @pl.when(k > 0)
        def _():
            remote(attended.at[k], heads.at[:, mine], so.at[k], ro.at[k], source).start()

        @pl.when(k == 0)
        def _():
            heads[:, mine] = attended[0]

        return 0

    lax.fori_loop(0, 16, one_block, 0)
    for d in (1, 2, 3):
        to_x(3)[d - 1].wait_recv()
        to_core(3, d).start()
    backs = [None]
    for k in range(1, 16):
        source = along((4 - ORDER[k][0]) % 4, (4 - ORDER[k][1]) % 4)
        mine = pl.ds(pl.multiple_of(me * 128, 128), 128)
        backs.append(remote(attended.at[k], heads.at[:, mine], so.at[k], ro.at[k], source))
    for k in range(1, 16):
        backs[k].wait_recv()
    for g in range(4):
        for d in range(4):
            to_core(g, d).wait_recv()

    @pl.loop(0, 8)
    def _(n):
        cols = pl.ds(pl.multiple_of(n * 256, 256), 256)
        p = jnp.dot(heads[...], wo[n].reshape(2048, 256), preferred_element_type=f32).astype(bf16)
        after[:, cols] = resid[:, cols].astype(f32) + p.astype(f32)

    @pl.loop(0, 8)
    def _(r):
        rows = pl.ds(pl.multiple_of(r * 32, 32), 32)
        a = after[rows, :]
        scale = lax.rsqrt(jnp.mean(a * a, axis=-1, keepdims=True) + epsilon)
        normed[rows, :] = (a * scale * gain[...]).astype(bf16)

    tok = lax.broadcasted_iota(i32, (256, 256), 0)
    tok_l = lax.broadcasted_iota(i32, (256, 256), 1)
    upper = jnp.where(tok < tok_l, 1.0, 0.0).astype(bf16)
    lower = jnp.where(tok_l < tok, 1.0, 0.0).astype(bf16)
    ex_t = lax.broadcasted_iota(i32, (16, 256), 0)
    hot_t = [jnp.where(ex_t == routes_t[k : k + 1, :], 1.0, 0.0) for k in range(2)]
    before_t = jnp.dot((hot_t[0] + hot_t[1]).astype(bf16), upper, preferred_element_type=f32)
    base_t = before_t + (ex_t * 64).astype(f32)
    slot_t = [jnp.sum(h * base_t, axis=0, keepdims=True).astype(i32) for h in hot_t]
    ex_c = lax.broadcasted_iota(i32, (256, 128), 1)
    hot_c = [jnp.where(ex_c == routes[:, k : k + 1], 1.0, 0.0) for k in range(2)]
    before_c = jnp.dot(lower, (hot_c[0] + hot_c[1]).astype(bf16), preferred_element_type=f32)
    base_c = before_c + (ex_c * 64).astype(f32)
    slot_c = [jnp.sum(h * base_c, axis=1, keepdims=True).astype(i32) for h in hot_c]

    def places(g, axis):
        shape = (256, 1) if axis == 0 else (1, 256)
        r = lax.broadcasted_iota(i32, shape, axis)
        owner = [shifted(me, *ORDER[4 * g + j]) * 64 for j in range(4)]
        base = jnp.where(r < 64, owner[0], jnp.where(r < 128, owner[1], jnp.where(r < 192, owner[2], owner[3])))
        return base + (r & 63)

    first = [
        None if k == 0 else remote(outgoing.at[k], arrived.at[k], send1.at[k], recv1.at[k], shifted(me, *ORDER[k]))
        for k in range(16)
    ]
    for g in range(4):
        place = places(g, 0)
        pick = jnp.where((slot_t[0] == place) | (slot_t[1] == place), 1.0, 0.0).astype(bf16)
        for n in range(4):
            cols = slice(n * 512, n * 512 + 512)
            rows = jnp.dot(pick, normed[:, cols], preferred_element_type=f32).astype(bf16)
            for j in range(4):
                k = 4 * g + j
                (arrived if k == 0 else outgoing)[k, :, cols] = rows[j * 64 : j * 64 + 64]
        if g > 0:
            for k in range(max(1, 4 * g - 4), 4 * g):
                first[k].start()
    for load in loads:
        load.wait()
    for k in range(12, 16):
        first[k].start()

    second = [
        None if k == 0 else remote(result.at[k], returned.at[k], send2.at[k], recv2.at[k], shifted(me, (4 - ORDER[k][0]) % 4, (4 - ORDER[k][1]) % 4))
        for k in range(16)
    ]
    for g in range(4):
        for k in range(max(1, 4 * g), 4 * g + 4):
            first[k].wait_recv()

        @pl.loop(0, 4)
        def _(n):
            cols = pl.ds(pl.multiple_of(n * 256, 256), 256)
            rows = arrived[4 * g : 4 * g + 4].reshape(256, 2048)
            gate = jnp.dot(rows, wg[:, cols], preferred_element_type=f32)
            up = jnp.dot(rows, wu[:, cols], preferred_element_type=f32)
            hidden[:, cols] = (gate / (1.0 + jnp.exp(-gate)) * up).astype(bf16)

        @pl.loop(0, 4)
        def _(n):
            cols = pl.ds(pl.multiple_of(n * 512, 512), 512)
            rows = jnp.dot(hidden[...], wd[:, cols], preferred_element_type=f32).astype(bf16)
            for j in range(4):
                k = 4 * g + j
                (returned if k == 0 else result)[k, :, cols] = rows[j * 64 : j * 64 + 64]

        for k in range(max(1, 4 * g), 4 * g + 4):
            second[k].start()

    for g in range(4):
        place = places(g, 1)
        picks = [jnp.where(s == place, 1.0, 0.0).astype(bf16) for s in slot_c]
        for k in range(max(1, 4 * g), 4 * g + 4):
            second[k].wait_recv()
        for n in range(4):
            cols = slice(n * 512, n * 512 + 512)
            rows = returned[4 * g : 4 * g + 4, :, cols].reshape(256, 512)
            t = weight[:, 0:1] * jnp.dot(picks[0], rows, preferred_element_type=f32)
            t = t + weight[:, 1:2] * jnp.dot(picks[1], rows, preferred_element_type=f32)
            if g > 0:
                t = t + total[:, cols]
            if g < 3:
                total[:, cols] = t
            else:
                out[:, cols] = (after[:, cols] + t).astype(bf16)
    for k in range(1, 16):
        first[k].wait_send()
        second[k].wait_send()
    for c in a1 + b1 + w1 + a2 + b2 + w2 + asks[1:] + backs[1:]:
        c.wait_send()
    for g in range(4):
        for c in to_x(g) + [to_core(g, d) for d in range(4)]:
            c.wait_send()


def layer(q_slab, lat_a, lat_b, up_kv, wo, resid, gain, routes, weight, wg, wu, wd):
    v, a = pl.BlockSpec(memory_space=pltpu.VMEM), pl.BlockSpec(memory_space=pl.ANY)
    bf16, f32 = jnp.bfloat16, jnp.float32
    dma = pltpu.SemaphoreType.DMA
    return pl.pallas_call(
        layer_kernel,
        name="layer",
        out_shape=jax.ShapeDtypeStruct((256, 2048), bf16),
        in_specs=[a, a, a, v, a] + [v] * 5 + [a] * 3,
        out_specs=v,
        scratch_shapes=[
            pltpu.VMEM((2048, 1024), bf16),
            pltpu.VMEM((2048, 1024), bf16),
            pltpu.VMEM((1024, 2048), bf16),
            pltpu.VMEM((256, 2048), f32),
            pltpu.VMEM((256, 2048), bf16),
            pltpu.VMEM((16, 64, 2048), bf16),
            pltpu.VMEM((16, 64, 2048), bf16),
            pltpu.VMEM((256, 1024), bf16),
            pltpu.VMEM((16, 64, 2048), bf16),
            pltpu.VMEM((16, 64, 2048), bf16),
            pltpu.VMEM((256, 2048), f32),
            pltpu.VMEM((16, 384, 128), bf16),
            pltpu.VMEM((4, 4, 256, 128), bf16),
            pltpu.VMEM((4, 4, 384, 128), bf16),
            pltpu.VMEM((4096, 256), bf16),
            pltpu.VMEM((4096, 256), bf16),
            pltpu.VMEM((256, 256), bf16),
            pltpu.VMEM((16, 256, 128), bf16),
            pltpu.VMEM((256, 2048), bf16),
            pltpu.VMEM((8, 4, 4, 128, 256), bf16),
            dma((3,)),
        ]
        + [dma((16,))] * 4
        + [dma((4,))] * 9
        + [dma((16,))] * 4
        + [dma((4,))] * 4
        + [dma((4, 4))] * 4,
        compiler_params=pltpu.CompilerParams(
            collective_id=1, has_side_effects=True, vmem_limit_bytes=65400 * 1024
        ),
    )(q_slab, lat_a, lat_b, up_kv, wo, resid, gain, routes, routes.T, weight, wg, wu, wd)


def shards(
    query_nope,
    query_rope,
    latent,
    key_rope,
    resid,
    latent_gain,
    key_up,
    value_up,
    out_proj,
    norm_gain,
    expert_gate,
    expert_up,
    expert_down,
    routes,
    route_weight,
):
    tokens = latent.shape[1]
    local_pos = lax.axis_index("sp") * tokens + jnp.arange(tokens, dtype=jnp.int32)
    latent_normed = rms_scaled(latent[0], latent_gain).astype(jnp.bfloat16)
    key_turned = rotate(key_rope[0], local_pos)
    query_turned = rotate(query_rope[0], local_pos)
    half = tokens // 2
    turned = query_turned.reshape(2, half, 16, 64).transpose(2, 1, 0, 3).reshape(16, half, 128)
    q_slab = jnp.concatenate([query_nope[0].transpose(1, 0, 2), turned], axis=1)
    key_pack = jnp.concatenate([key_turned[:half], key_turned[half:]], axis=1)
    lat_a = latent_normed[:, :128]
    lat_b = jnp.concatenate([latent_normed[:, 128:], key_pack], axis=0)
    up_kv = jnp.concatenate([key_up, value_up], axis=1)
    return layer(
        q_slab, lat_a, lat_b, up_kv, out_proj, resid[0], norm_gain[None], routes[0], route_weight[0],
        expert_gate[0], expert_up[0], expert_down[0],
    )[None]


def solution(mesh):
    return jax.shard_map(
        shards,
        mesh=mesh,
        in_specs=(
            P("dp", "sp", None, None),
            P("dp", "sp", None, None),
            P("dp", "sp", None),
            P("dp", "sp", None),
            P("dp", "sp", None),
            P(),
            P(None, "sp"),
            P(None, "sp"),
            P("sp", "dp"),
            P(),
            P("sp", None, None),
            P("sp", None, None),
            P("sp", None, None),
            P("dp", "sp", None),
            P("dp", "sp", None),
        ),
        out_specs=P("dp", "sp", None),
        check_vma=False,
    )
```

```python
import math

import jax
import jax.numpy as jnp
from jax import lax
from jax.experimental import pallas as pl
from jax.experimental.pallas import tpu as pltpu
from jax.sharding import PartitionSpec as P

epsilon = 1e-06
rope_base = 10000.0
masked_score = -1e30


def rotate(values, positions):
    half_width = values.shape[-1] // 2
    frequency = rope_base ** (-jnp.arange(half_width, dtype=jnp.float32) / half_width)
    angles = positions.astype(jnp.float32)[:, None] * frequency[None, :]
    cosine = jnp.cos(angles)
    sine_part = jnp.sin(angles)
    if values.ndim == 3:
        cosine = cosine[:, None, :]
        sine_part = sine_part[:, None, :]
    floats = values.astype(jnp.float32)
    first_half = floats[..., :half_width]
    second_half = floats[..., half_width:]
    turned = jnp.concatenate(
        [
            first_half * cosine - second_half * sine_part,
            second_half * cosine + first_half * sine_part,
        ],
        axis=-1,
    )
    return turned.astype(jnp.bfloat16)


def rms_scaled(values, gain):
    floats = values.astype(jnp.float32)
    return floats * lax.rsqrt(jnp.mean(floats * floats, axis=-1, keepdims=True) + epsilon) * gain


ORDER = [(0, 0), (2, 2), (3, 2), (2, 3), (1, 2), (2, 1), (0, 2), (2, 0), (3, 1), (1, 3), (3, 3), (1, 1), (3, 0), (0, 3), (1, 0), (0, 1)]
MESH = pl.DeviceIdType.MESH


def packed(digits):
    value = sum(d << (2 * i) for i, d in enumerate(digits))
    return value - (1 << 32) if value >= 1 << 31 else value


PAIRS = [(0, 0), (2, 1), (1, 1), (3, 1), (2, 0), (0, 1), (1, 0), (3, 0)]
PZ, PJ = packed([o[0] for o in PAIRS]), packed([o[1] for o in PAIRS])


def shifted(me, dz, dy):
    z, y = me // 4, lax.rem(me, 4)
    return lax.rem(z + dz, 4) * 4 + lax.rem(y + dy, 4)


def remote(src, dst, send, recv, target):
    return pltpu.make_async_remote_copy(
        src_ref=src,
        dst_ref=dst,
        send_sem=send,
        recv_sem=recv,
        device_id={"sp": target},
        device_id_type=MESH,
    )


def layer_kernel(
    q_in_hbm, lat_a, lat_b, up_k, up_vt, wo_hbm, resid, gain, routes, routes_t, weight, wg_hbm, wu_hbm, wd_hbm, out,
    wg, wu, wd, after, normed, outgoing, arrived, hidden, result, returned, total,
    q_in, la, lb, keys, vals, attended, heads, wo,
    wsem, send1, recv1, send2, recv2,
    lsem, sa1, ra1, sb1, rb1, sa2, ra2, sb2, rb2, sq, rq, so, ro, swz, rwz, swy, rwy, swx, rwx, swc, rwc,
):
    me, dp = lax.axis_index("sp"), lax.axis_index("dp")
    z, y = me // 4, lax.rem(me, 4)
    x, core = dp // 2, lax.rem(dp, 2)
    f32, bf16, i32 = jnp.float32, jnp.bfloat16, jnp.int32
    barrier = pltpu.get_barrier_semaphore()
    for dz, dy in ORDER[1:]:
        pl.semaphore_signal(barrier, inc=1, device_id={"sp": shifted(me, dz, dy)}, device_id_type=MESH)
    x_peer = [None] + [lax.rem(x + d, 4) * 2 + core for d in (1, 2, 3)]
    x_from = [dp] + [lax.rem(x + 4 - d, 4) * 2 + core for d in (1, 2, 3)]
    other = x * 2 + 1 - core
    for t in x_peer[1:] + [other]:
        pl.semaphore_signal(barrier, inc=1, device_id={"dp": t}, device_id_type=MESH)
    fill_wo = pltpu.make_async_copy(wo_hbm, wo.at[dp, z, y], lsem.at[0])
    fill_wo.start()
    fill_q = pltpu.make_async_copy(q_in_hbm.at[me], q_in.at[me], lsem.at[1])
    fill_q.start()
    fill_a = pltpu.make_async_copy(lat_a, la.at[z, y], lsem.at[2])
    fill_a.start()
    fill_b = pltpu.make_async_copy(lat_b, lb.at[z, y], lsem.at[3])
    fill_b.start()
    loads = [
        pltpu.make_async_copy(a, b, wsem.at[i])
        for i, (a, b) in enumerate(((wg_hbm, wg), (wu_hbm, wu), (wd_hbm, wd)))
    ]
    for load in loads:
        load.start()
    fill_a.wait()
    fill_b.wait()
    fill_wo.wait()
    pl.semaphore_wait(barrier, 19)

    def along(dz, dy):
        return shifted(me, dz, dy)

    a1 = [remote(la.at[z, y], la.at[z, y], sa1.at[d], ra1.at[d], along(d, 0)) for d in (1, 2, 3)]
    b1 = [remote(lb.at[z, y], lb.at[z, y], sb1.at[d], rb1.at[d], along(0, d)) for d in (1, 2, 3)]
    w1 = [remote(wo.at[dp, z, y], wo.at[dp, z, y], swz.at[d], rwz.at[d], along(d, 0)) for d in (1, 2, 3)]
    a2 = [remote(la.at[:, y], la.at[:, y], sa2.at[d], ra2.at[d], along(0, d)) for d in (1, 2, 3)]
    b2 = [remote(lb.at[z], lb.at[z], sb2.at[d], rb2.at[d], along(d, 0)) for d in (1, 2, 3)]
    w2 = [remote(wo.at[dp, :, y], wo.at[dp, :, y], swy.at[d], rwy.at[d], along(0, d)) for d in (1, 2, 3)]
    asks = []
    for r, (dz, dj) in enumerate(PAIRS):
        for e in range(2):
            if r == 0:
                target = me + 1 - 2 * lax.rem(y, 2)
                if e == 1:
                    continue
            else:
                target = lax.rem(z + 4 - dz, 4) * 4 + lax.rem(y // 2 + dj, 2) * 2 + e
            asks.append(remote(q_in_hbm.at[target], q_in.at[me], sq.at[2 * r + e], rq.at[me], target))

    def to_x(g):
        part = wo.at[dp, :, lax.rem(y + 4 - g, 4)]
        copies = [
            pltpu.make_async_remote_copy(
                src_ref=part, dst_ref=part, send_sem=swx.at[g, d], recv_sem=rwx.at[g, d],
                device_id={"dp": x_peer[d]}, device_id_type=MESH,
            )
            for d in (1, 2, 3)
        ]
        return copies

    def to_core(g, d):
        part = wo.at[x_from[d], :, lax.rem(y + 4 - g, 4)]
        return pltpu.make_async_remote_copy(
            src_ref=part, dst_ref=part, send_sem=swc.at[g, d], recv_sem=rwc.at[g, d],
            device_id={"dp": other}, device_id_type=MESH,
        )

    for c in w1 + a1 + b1:
        c.start()
    for c in w1:
        c.wait_recv()
    for c in w2 + to_x(0) + [to_core(0, 0)]:
        c.start()
    for c in a1:
        c.wait_recv()
    for c in a2:
        c.start()
    for c in b1:
        c.wait_recv()
    for c in b2 + asks:
        c.start()
    for g in (1, 2, 3):
        w2[g - 1].wait_recv()
        for c in to_x(g) + [to_core(g, 0)]:
            c.start()

    vals[128:144, :] = jnp.ones((16, 4096), bf16)
    for c in a2 + b2:
        c.wait_recv()

    @pl.loop(0, 16)
    def _(b):
        bz, by = b // 4, lax.rem(b, 4)
        rows = pl.ds(pl.multiple_of(b * 256, 256), 256)
        lat = jnp.concatenate([la[bz, by], lb[bz, by, 0:256, :]], axis=1)
        keys[rows, 0:128] = jnp.dot(lat, up_k[...], preferred_element_type=f32).astype(bf16)
        vals[0:128, rows] = lax.dot_general(
            up_vt[...], lat, (((1,), (1,)), ((), ())), preferred_element_type=f32
        ).astype(bf16)
        turn = lb[bz, by, 256:384, :].astype(f32)
        swap = pltpu.roll(turn, 64, 1)
        low = lax.broadcasted_iota(i32, (128, 128), 1) < 64
        start = pl.multiple_of(b * 256, 256)
        keys[pl.ds(start, 128), 128:256] = jnp.where(low, turn, swap).astype(bf16)
        keys[pl.ds(pl.multiple_of(start + 128, 128), 128), 128:256] = jnp.where(low, swap, turn).astype(bf16)

    fill_q.wait()
    unit = 192.0 ** -0.5 * math.log2(math.e)
    mine = pl.ds(pl.multiple_of(me * 128, 128), 128)

    def one_pair(r, _):
        dz, dj = (PZ >> (2 * r)) & 3, (PJ >> (2 * r)) & 3
        pair = lax.rem(z + dz, 4) * 2 + lax.rem(y // 2 + dj, 2)
        for e in range(2):
            source = 2 * pair + e

            @pl.when(source != me)
            def _(source=source):
                remote(q_in.at[source], q_in.at[source], sq.at[0], rq.at[source], source).wait_recv()

        for g in (0, 1, 2):

            @pl.when(r == 2 * g + 2)
            def _(g=g):
                for d in (1, 2, 3):
                    to_x(g)[d - 1].wait_recv()
                    to_core(g, d).start()

        q = jnp.concatenate([q_in[2 * pair], q_in[2 * pair + 1]], axis=1)

        def scores(at):
            return jnp.dot(keys[pl.ds(at, 512), 0:192], q, preferred_element_type=f32)

        def weigh(s, at, top, acc):
            new = jnp.maximum(top, jnp.max(s, axis=0, keepdims=True) * unit)
            p = jnp.exp2(s * unit - new).astype(bf16)
            return new, acc * jnp.exp2(top - new) + jnp.dot(
                vals[:, pl.ds(at, 512)], p, preferred_element_type=f32
            )

        last = pl.multiple_of(pair * 512, 512)
        key_id = lax.broadcasted_iota(i32, (512, 512), 0)
        row_id = lax.broadcasted_iota(i32, (512, 512), 1)
        s = jnp.where(key_id <= row_id, scores(last), masked_score)
        top = jnp.max(s, axis=0, keepdims=True) * unit
        p = jnp.exp2(s * unit - top).astype(bf16)
        acc = jnp.dot(vals[:, pl.ds(last, 512)], p, preferred_element_type=f32)

        def single(i, carry):
            at = pl.multiple_of((pair - 1) * 512, 512)
            return weigh(scores(at), at, *carry)

        def double(i, carry):
            at = pl.multiple_of(i * 1024, 1024)
            then = pl.multiple_of(at + 512, 512)
            s, t = scores(at), scores(then)
            return weigh(t, then, *weigh(s, at, *carry))

        carry = lax.fori_loop(0, lax.rem(pair, 2), single, (top, acc))
        top, acc = lax.fori_loop(0, pair // 2, double, carry)
        rows = acc[0:128] / acc[128:129]
        for e in range(2):
            attended[2 * r + e] = rows[:, 256 * e : 256 * e + 256].T.astype(bf16)
        for e in range(2):
            source = 2 * pair + e

            @pl.when(source != me)
            def _(e=e, source=source):
                remote(attended.at[2 * r + e], heads.at[:, mine], so.at[2 * r + e], ro.at[me], source).start()

            @pl.when(source == me)
            def _(e=e):
                heads[:, mine] = attended[2 * r + e]

        return 0

    lax.fori_loop(0, 8, one_pair, 0)
    for d in (1, 2, 3):
        to_x(3)[d - 1].wait_recv()
        to_core(3, d).start()
    for k in range(1, 16):
        head = along(*ORDER[k])
        there = pl.ds(pl.multiple_of(head * 128, 128), 128)
        remote(attended.at[0], heads.at[:, there], so.at[0], ro.at[head], head).wait_recv()
    for g in range(4):
        for d in range(4):
            to_core(g, d).wait_recv()

    @pl.loop(0, 8)
    def _(n):
        cols = pl.ds(pl.multiple_of(n * 256, 256), 256)
        p = jnp.dot(heads[...], wo[n].reshape(2048, 256), preferred_element_type=f32).astype(bf16)
        after[:, cols] = resid[:, cols].astype(f32) + p.astype(f32)

    @pl.loop(0, 8)
    def _(r):
        rows = pl.ds(pl.multiple_of(r * 32, 32), 32)
        a = after[rows, :]
        scale = lax.rsqrt(jnp.mean(a * a, axis=-1, keepdims=True) + epsilon)
        normed[rows, :] = (a * scale * gain[...]).astype(bf16)

    tok = lax.broadcasted_iota(i32, (256, 256), 0)
    tok_l = lax.broadcasted_iota(i32, (256, 256), 1)
    upper = jnp.where(tok < tok_l, 1.0, 0.0).astype(bf16)
    lower = jnp.where(tok_l < tok, 1.0, 0.0).astype(bf16)
    ex_t = lax.broadcasted_iota(i32, (16, 256), 0)
    hot_t = [jnp.where(ex_t == routes_t[k : k + 1, :], 1.0, 0.0) for k in range(2)]
    before_t = jnp.dot((hot_t[0] + hot_t[1]).astype(bf16), upper, preferred_element_type=f32)
    base_t = before_t + (ex_t * 64).astype(f32)
    slot_t = [jnp.sum(h * base_t, axis=0, keepdims=True).astype(i32) for h in hot_t]
    ex_c = lax.broadcasted_iota(i32, (256, 128), 1)
    hot_c = [jnp.where(ex_c == routes[:, k : k + 1], 1.0, 0.0) for k in range(2)]
    before_c = jnp.dot(lower, (hot_c[0] + hot_c[1]).astype(bf16), preferred_element_type=f32)
    base_c = before_c + (ex_c * 64).astype(f32)
    slot_c = [jnp.sum(h * base_c, axis=1, keepdims=True).astype(i32) for h in hot_c]

    def places(g, axis):
        shape = (256, 1) if axis == 0 else (1, 256)
        r = lax.broadcasted_iota(i32, shape, axis)
        owner = [shifted(me, *ORDER[4 * g + j]) * 64 for j in range(4)]
        base = jnp.where(r < 64, owner[0], jnp.where(r < 128, owner[1], jnp.where(r < 192, owner[2], owner[3])))
        return base + (r & 63)

    first = [
        None if k == 0 else remote(outgoing.at[k], arrived.at[k], send1.at[k], recv1.at[k], shifted(me, *ORDER[k]))
        for k in range(16)
    ]
    for g in range(4):
        place = places(g, 0)
        pick = jnp.where((slot_t[0] == place) | (slot_t[1] == place), 1.0, 0.0).astype(bf16)
        for n in range(4):
            cols = slice(n * 512, n * 512 + 512)
            rows = jnp.dot(pick, normed[:, cols], preferred_element_type=f32).astype(bf16)
            for j in range(4):
                k = 4 * g + j
                (arrived if k == 0 else outgoing)[k, :, cols] = rows[j * 64 : j * 64 + 64]
        if g > 0:
            for k in range(max(1, 4 * g - 4), 4 * g):
                first[k].start()
    for load in loads:
        load.wait()
    for k in range(12, 16):
        first[k].start()

    second = [
        None if k == 0 else remote(result.at[k], returned.at[k], send2.at[k], recv2.at[k], shifted(me, (4 - ORDER[k][0]) % 4, (4 - ORDER[k][1]) % 4))
        for k in range(16)
    ]
    for g in range(4):
        for k in range(max(1, 4 * g), 4 * g + 4):
            first[k].wait_recv()

        @pl.loop(0, 4)
        def _(n):
            cols = pl.ds(pl.multiple_of(n * 256, 256), 256)
            rows = arrived[4 * g : 4 * g + 4].reshape(256, 2048)
            gate = jnp.dot(rows, wg[:, cols], preferred_element_type=f32)
            up = jnp.dot(rows, wu[:, cols], preferred_element_type=f32)
            hidden[:, cols] = (gate / (1.0 + jnp.exp(-gate)) * up).astype(bf16)

        @pl.loop(0, 4)
        def _(n):
            cols = pl.ds(pl.multiple_of(n * 512, 512), 512)
            rows = jnp.dot(hidden[...], wd[:, cols], preferred_element_type=f32).astype(bf16)
            for j in range(4):
                k = 4 * g + j
                (returned if k == 0 else result)[k, :, cols] = rows[j * 64 : j * 64 + 64]

        for k in range(max(1, 4 * g), 4 * g + 4):
            second[k].start()

    for g in range(4):
        place = places(g, 1)
        picks = [jnp.where(s == place, 1.0, 0.0).astype(bf16) for s in slot_c]
        for k in range(max(1, 4 * g), 4 * g + 4):
            second[k].wait_recv()
        for n in range(4):
            cols = slice(n * 512, n * 512 + 512)
            rows = returned[4 * g : 4 * g + 4, :, cols].reshape(256, 512)
            t = weight[:, 0:1] * jnp.dot(picks[0], rows, preferred_element_type=f32)
            t = t + weight[:, 1:2] * jnp.dot(picks[1], rows, preferred_element_type=f32)
            if g > 0:
                t = t + total[:, cols]
            if g < 3:
                total[:, cols] = t
            else:
                out[:, cols] = (after[:, cols] + t).astype(bf16)
    for k in range(1, 16):
        first[k].wait_send()
        second[k].wait_send()
    for c in a1 + b1 + w1 + a2 + b2 + w2 + asks:
        c.wait_send()
    for n in range(16):

        @pl.when(lax.rem(y, 2) != n)
        def _(n=n):
            remote(attended.at[n], heads.at[:, mine], so.at[n], ro.at[me], me).wait_send()

    for g in range(4):
        for c in to_x(g) + [to_core(g, d) for d in range(4)]:
            c.wait_send()


def layer(q_slab, lat_a, lat_b, up_k, up_vt, wo, resid, gain, routes, weight, wg, wu, wd):
    v, a = pl.BlockSpec(memory_space=pltpu.VMEM), pl.BlockSpec(memory_space=pl.ANY)
    bf16, f32 = jnp.bfloat16, jnp.float32
    dma = pltpu.SemaphoreType.DMA
    return pl.pallas_call(
        layer_kernel,
        name="layer",
        out_shape=jax.ShapeDtypeStruct((256, 2048), bf16),
        in_specs=[a, a, a, v, v, a] + [v] * 5 + [a] * 3,
        out_specs=v,
        scratch_shapes=[
            pltpu.VMEM((2048, 1024), bf16),
            pltpu.VMEM((2048, 1024), bf16),
            pltpu.VMEM((1024, 2048), bf16),
            pltpu.VMEM((256, 2048), f32),
            pltpu.VMEM((256, 2048), bf16),
            pltpu.VMEM((16, 64, 2048), bf16),
            pltpu.VMEM((16, 64, 2048), bf16),
            pltpu.VMEM((256, 1024), bf16),
            pltpu.VMEM((16, 64, 2048), bf16),
            pltpu.VMEM((16, 64, 2048), bf16),
            pltpu.VMEM((256, 2048), f32),
            pltpu.VMEM((16, 192, 256), bf16),
            pltpu.VMEM((4, 4, 256, 128), bf16),
            pltpu.VMEM((4, 4, 384, 128), bf16),
            pltpu.VMEM((4096, 256), bf16),
            pltpu.VMEM((144, 4096), bf16),
            pltpu.VMEM((16, 256, 128), bf16),
            pltpu.VMEM((256, 2048), bf16),
            pltpu.VMEM((8, 4, 4, 128, 256), bf16),
            dma((3,)),
        ]
        + [dma((16,))] * 4
        + [dma((4,))] * 9
        + [dma((16,))] * 4
        + [dma((4,))] * 4
        + [dma((4, 4))] * 4,
        compiler_params=pltpu.CompilerParams(
            collective_id=1, has_side_effects=True, vmem_limit_bytes=65400 * 1024
        ),
    )(q_slab, lat_a, lat_b, up_k, up_vt, wo, resid, gain, routes, routes.T, weight, wg, wu, wd)


def shards(
    query_nope,
    query_rope,
    latent,
    key_rope,
    resid,
    latent_gain,
    key_up,
    value_up,
    out_proj,
    norm_gain,
    expert_gate,
    expert_up,
    expert_down,
    routes,
    route_weight,
):
    tokens = latent.shape[1]
    local_pos = lax.axis_index("sp") * tokens + jnp.arange(tokens, dtype=jnp.int32)
    latent_normed = rms_scaled(latent[0], latent_gain).astype(jnp.bfloat16)
    key_turned = rotate(key_rope[0], local_pos)
    query_turned = rotate(query_rope[0], local_pos)
    half = tokens // 2
    q_slab = jnp.concatenate(
        [query_nope[0].transpose(1, 2, 0), query_turned.transpose(1, 2, 0)], axis=1
    )
    key_pack = jnp.concatenate([key_turned[:half], key_turned[half:]], axis=1)
    lat_a = latent_normed[:, :128]
    lat_b = jnp.concatenate([latent_normed[:, 128:], key_pack], axis=0)
    return layer(
        q_slab, lat_a, lat_b, key_up, value_up.T, out_proj, resid[0], norm_gain[None], routes[0], route_weight[0],
        expert_gate[0], expert_up[0], expert_down[0],
    )[None]


def solution(mesh):
    return jax.shard_map(
        shards,
        mesh=mesh,
        in_specs=(
            P("dp", "sp", None, None),
            P("dp", "sp", None, None),
            P("dp", "sp", None),
            P("dp", "sp", None),
            P("dp", "sp", None),
            P(),
            P(None, "sp"),
            P(None, "sp"),
            P("sp", "dp"),
            P(),
            P("sp", None, None),
            P("sp", None, None),
            P("sp", None, None),
            P("dp", "sp", None),
            P("dp", "sp", None),
        ),
        out_specs=P("dp", "sp", None),
        check_vma=False,
    )
```

```python
import math

import jax
import jax.numpy as jnp
from jax import lax
from jax.experimental import pallas as pl
from jax.experimental.pallas import tpu as pltpu
from jax.sharding import PartitionSpec as P

epsilon = 1e-06
rope_base = 10000.0
masked_score = -1e30


def rotate(values, positions):
    half_width = values.shape[-1] // 2
    frequency = rope_base ** (-jnp.arange(half_width, dtype=jnp.float32) / half_width)
    angles = positions.astype(jnp.float32)[:, None] * frequency[None, :]
    cosine = jnp.cos(angles)
    sine_part = jnp.sin(angles)
    if values.ndim == 3:
        cosine = cosine[:, None, :]
        sine_part = sine_part[:, None, :]
    floats = values.astype(jnp.float32)
    first_half = floats[..., :half_width]
    second_half = floats[..., half_width:]
    turned = jnp.concatenate(
        [
            first_half * cosine - second_half * sine_part,
            second_half * cosine + first_half * sine_part,
        ],
        axis=-1,
    )
    return turned.astype(jnp.bfloat16)


def rms_scaled(values, gain):
    floats = values.astype(jnp.float32)
    return floats * lax.rsqrt(jnp.mean(floats * floats, axis=-1, keepdims=True) + epsilon) * gain


ORDER = [(0, 0), (2, 2), (3, 2), (2, 3), (1, 2), (2, 1), (0, 2), (2, 0), (3, 1), (1, 3), (3, 3), (1, 1), (3, 0), (0, 3), (1, 0), (0, 1)]
MESH = pl.DeviceIdType.MESH


def packed(digits):
    value = sum(d << (2 * i) for i, d in enumerate(digits))
    return value - (1 << 32) if value >= 1 << 31 else value


PLACE = {0: 0, 1: 1, 3: 2, 2: 3}
SHIFT = [0, 1, 3, 2]
PAIRS = [(0, 0), (2, 1), (1, 1), (3, 1), (2, 0), (0, 1), (1, 0), (3, 0)]
PZ, PJ = packed([o[0] for o in PAIRS]), packed([o[1] for o in PAIRS])


def shifted(me, dz, dy):
    z, y = me // 4, lax.rem(me, 4)
    return lax.rem(z + dz, 4) * 4 + lax.rem(y + dy, 4)


def remote(src, dst, send, recv, target):
    return pltpu.make_async_remote_copy(
        src_ref=src,
        dst_ref=dst,
        send_sem=send,
        recv_sem=recv,
        device_id={"sp": target},
        device_id_type=MESH,
    )


def layer_kernel(
    q_in_hbm, lat_a, lat_b, up_k, up_vt, wo_hbm, resid, gain, told_in, wg_hbm, wu_hbm, wd_hbm, out,
    wg, wu, wd, after, told_all, shared, outgoing, arrived, hidden, result, returned, final,
    q_in, la, lb, keys, vals, attended, heads, wo,
    wsem, st, rt, ssh, rsh, sd, rd, sg, rg, sf, rf,
    lsem, sa1, ra1, sb1, rb1, sa2, ra2, sb2, rb2, sq, rq, so, ro, swz, rwz, swy, rwy, swx, rwx, swc, rwc,
):
    me, dp = lax.axis_index("sp"), lax.axis_index("dp")
    z, y = me // 4, lax.rem(me, 4)
    x, core = dp // 2, lax.rem(dp, 2)
    f32, bf16, i32 = jnp.float32, jnp.bfloat16, jnp.int32
    barrier = pltpu.get_barrier_semaphore()
    for dz, dy in ORDER[1:]:
        pl.semaphore_signal(barrier, inc=1, device_id={"sp": shifted(me, dz, dy)}, device_id_type=MESH)
    x_peer = [None] + [lax.rem(x + d, 4) * 2 + core for d in (1, 2, 3)]
    x_from = [dp] + [lax.rem(x + 4 - d, 4) * 2 + core for d in (1, 2, 3)]
    other = x * 2 + 1 - core
    for t in x_peer[1:] + [other]:
        pl.semaphore_signal(barrier, inc=1, device_id={"dp": t}, device_id_type=MESH)
    fill_wo = pltpu.make_async_copy(wo_hbm, wo.at[dp, z, y], lsem.at[0])
    fill_wo.start()
    fill_q = pltpu.make_async_copy(q_in_hbm.at[me], q_in.at[me], lsem.at[1])
    fill_q.start()
    fill_a = pltpu.make_async_copy(lat_a, la.at[z, y], lsem.at[2])
    fill_a.start()
    fill_b = pltpu.make_async_copy(lat_b, lb.at[z, y], lsem.at[3])
    fill_b.start()
    loads = [
        pltpu.make_async_copy(a, b, wsem.at[i])
        for i, (a, b) in enumerate(((wg_hbm, wg), (wu_hbm, wu), (wd_hbm, wd)))
    ]
    for load in loads:
        load.start()
    tok = lax.broadcasted_iota(i32, (256, 256), 0)
    tok_l = lax.broadcasted_iota(i32, (256, 256), 1)
    upper = jnp.where(tok < tok_l, 1.0, 0.0).astype(bf16)
    expert = lax.broadcasted_iota(i32, (16, 256), 0).astype(f32)
    hot = [jnp.where(expert == told_in[k : k + 1, :], 1.0, 0.0) for k in range(2)]
    before = jnp.dot((hot[0] + hot[1]).astype(bf16), upper, preferred_element_type=f32) + expert * 64.0
    for h in range(2):
        for k in range(2):
            told_all[h, 0, k : k + 1, :] = jnp.sum(hot[k] * before, axis=0, keepdims=True)
        told_all[h, 0, 2:8, :] = told_in[2:8, :]
    fill_a.wait()
    fill_b.wait()
    fill_wo.wait()
    pl.semaphore_wait(barrier, 19)

    def along(dz, dy):
        return shifted(me, dz, dy)

    told = []
    for h in range(2):
        for d in (1, 2, 3):
            target = along(0, d) if h == 0 else along(d, 0)
            told.append(remote(told_all.at[h, 0], told_all.at[h, PLACE[d]], st.at[4 * h + d], rt.at[4 * h + d], target))
    a1 = [remote(la.at[z, y], la.at[z, y], sa1.at[d], ra1.at[d], along(d, 0)) for d in (1, 2, 3)]
    b1 = [remote(lb.at[z, y], lb.at[z, y], sb1.at[d], rb1.at[d], along(0, d)) for d in (1, 2, 3)]
    w1 = [remote(wo.at[dp, z, y], wo.at[dp, z, y], swz.at[d], rwz.at[d], along(d, 0)) for d in (1, 2, 3)]
    a2 = [remote(la.at[:, y], la.at[:, y], sa2.at[d], ra2.at[d], along(0, d)) for d in (1, 2, 3)]
    b2 = [remote(lb.at[z], lb.at[z], sb2.at[d], rb2.at[d], along(d, 0)) for d in (1, 2, 3)]
    w2 = [remote(wo.at[dp, :, y], wo.at[dp, :, y], swy.at[d], rwy.at[d], along(0, d)) for d in (1, 2, 3)]
    asks = []
    for r, (dz, dj) in enumerate(PAIRS):
        for e in range(2):
            if r == 0:
                target = me + 1 - 2 * lax.rem(y, 2)
                if e == 1:
                    continue
            else:
                target = lax.rem(z + 4 - dz, 4) * 4 + lax.rem(y // 2 + dj, 2) * 2 + e
            asks.append(remote(q_in_hbm.at[target], q_in.at[me], sq.at[2 * r + e], rq.at[me], target))

    def to_x(g):
        part = wo.at[dp, :, lax.rem(y + 4 - g, 4)]
        copies = [
            pltpu.make_async_remote_copy(
                src_ref=part, dst_ref=part, send_sem=swx.at[g, d], recv_sem=rwx.at[g, d],
                device_id={"dp": x_peer[d]}, device_id_type=MESH,
            )
            for d in (1, 2, 3)
        ]
        return copies

    def to_core(g, d):
        part = wo.at[x_from[d], :, lax.rem(y + 4 - g, 4)]
        return pltpu.make_async_remote_copy(
            src_ref=part, dst_ref=part, send_sem=swc.at[g, d], recv_sem=rwc.at[g, d],
            device_id={"dp": other}, device_id_type=MESH,
        )

    for c in w1 + a1 + b1:
        c.start()
    for c in w1:
        c.wait_recv()
    for c in w2 + to_x(0) + [to_core(0, 0)]:
        c.start()
    for c in a1:
        c.wait_recv()
    for c in a2:
        c.start()
    for c in b1:
        c.wait_recv()
    for c in b2 + told + asks:
        c.start()
    for g in (1, 2, 3):
        w2[g - 1].wait_recv()
        for c in to_x(g) + [to_core(g, 0)]:
            c.start()

    vals[128:144, :] = jnp.ones((16, 4096), bf16)
    for c in a2 + b2:
        c.wait_recv()

    @pl.loop(0, 16)
    def _(b):
        bz, by = b // 4, lax.rem(b, 4)
        rows = pl.ds(pl.multiple_of(b * 256, 256), 256)
        lat = jnp.concatenate([la[bz, by], lb[bz, by, 0:256, :]], axis=1)
        keys[rows, 0:128] = jnp.dot(lat, up_k[...], preferred_element_type=f32).astype(bf16)
        vals[0:128, rows] = lax.dot_general(
            up_vt[...], lat, (((1,), (1,)), ((), ())), preferred_element_type=f32
        ).astype(bf16)
        turn = lb[bz, by, 256:384, :].astype(f32)
        swap = pltpu.roll(turn, 64, 1)
        low = lax.broadcasted_iota(i32, (128, 128), 1) < 64
        start = pl.multiple_of(b * 256, 256)
        keys[pl.ds(start, 128), 128:256] = jnp.where(low, turn, swap).astype(bf16)
        keys[pl.ds(pl.multiple_of(start + 128, 128), 128), 128:256] = jnp.where(low, swap, turn).astype(bf16)

    fill_q.wait()
    unit = 192.0 ** -0.5 * math.log2(math.e)
    mine = pl.ds(pl.multiple_of(me * 128, 128), 128)

    def one_pair(r, _):
        dz, dj = (PZ >> (2 * r)) & 3, (PJ >> (2 * r)) & 3
        pair = lax.rem(z + dz, 4) * 2 + lax.rem(y // 2 + dj, 2)
        for e in range(2):
            source = 2 * pair + e

            @pl.when(source != me)
            def _(source=source):
                remote(q_in.at[source], q_in.at[source], sq.at[0], rq.at[source], source).wait_recv()

        for g in (0, 1, 2):

            @pl.when(r == 2 * g + 2)
            def _(g=g):
                for d in (1, 2, 3):
                    to_x(g)[d - 1].wait_recv()
                    to_core(g, d).start()

        q = jnp.concatenate([q_in[2 * pair], q_in[2 * pair + 1]], axis=1)

        def scores(at):
            return jnp.dot(keys[pl.ds(at, 512), 0:192], q, preferred_element_type=f32)

        def weigh(s, at, top, acc):
            new = jnp.maximum(top, jnp.max(s, axis=0, keepdims=True) * unit)
            p = jnp.exp2(s * unit - new).astype(bf16)
            return new, acc * jnp.exp2(top - new) + jnp.dot(
                vals[:, pl.ds(at, 512)], p, preferred_element_type=f32
            )

        last = pl.multiple_of(pair * 512, 512)
        key_id = lax.broadcasted_iota(i32, (512, 512), 0)
        row_id = lax.broadcasted_iota(i32, (512, 512), 1)
        s = jnp.where(key_id <= row_id, scores(last), masked_score)
        top = jnp.max(s, axis=0, keepdims=True) * unit
        p = jnp.exp2(s * unit - top).astype(bf16)
        acc = jnp.dot(vals[:, pl.ds(last, 512)], p, preferred_element_type=f32)

        def single(i, carry):
            at = pl.multiple_of((pair - 1) * 512, 512)
            return weigh(scores(at), at, *carry)

        def double(i, carry):
            at = pl.multiple_of(i * 1024, 1024)
            then = pl.multiple_of(at + 512, 512)
            s, t = scores(at), scores(then)
            return weigh(t, then, *weigh(s, at, *carry))

        carry = lax.fori_loop(0, lax.rem(pair, 2), single, (top, acc))
        top, acc = lax.fori_loop(0, pair // 2, double, carry)
        rows = acc[0:128] / acc[128:129]
        for e in range(2):
            attended[2 * r + e] = rows[:, 256 * e : 256 * e + 256].T.astype(bf16)
        for e in range(2):
            source = 2 * pair + e

            @pl.when(source != me)
            def _(e=e, source=source):
                remote(attended.at[2 * r + e], heads.at[:, mine], so.at[2 * r + e], ro.at[me], source).start()

            @pl.when(source == me)
            def _(e=e):
                heads[:, mine] = attended[2 * r + e]

        return 0

    lax.fori_loop(0, 8, one_pair, 0)
    for d in (1, 2, 3):
        to_x(3)[d - 1].wait_recv()
        to_core(3, d).start()
    for k in range(1, 16):
        head = along(*ORDER[k])
        there = pl.ds(pl.multiple_of(head * 128, 128), 128)
        remote(attended.at[0], heads.at[:, there], so.at[0], ro.at[head], head).wait_recv()
    for g in range(4):
        for d in range(4):
            to_core(g, d).wait_recv()

    @pl.loop(0, 8)
    def _(n):
        cols = pl.ds(pl.multiple_of(n * 256, 256), 256)
        p = jnp.dot(heads[...], wo[n].reshape(2048, 256), preferred_element_type=f32).astype(bf16)
        after[:, cols] = resid[:, cols].astype(f32) + p.astype(f32)

    @pl.loop(0, 8)
    def _(r):
        rows = pl.ds(pl.multiple_of(r * 32, 32), 32)
        a = after[rows, :]
        scale = lax.rsqrt(jnp.mean(a * a, axis=-1, keepdims=True) + epsilon)
        full = (a * scale * gain[...]).astype(bf16)
        shared[0, 0, rows, :] = full[:, 0:1024]
        shared[1, 0, rows, :] = full[:, 1024:2048]

    def line(h, d):
        return along(0, d) if h == 0 else along(d, 0)

    def cross(h, d):
        return along(d, 0) if h == 0 else along(0, d)

    def slots_of(h):
        r = lax.broadcasted_iota(i32, (256, 1), 0)
        owner = [cross(h, d) * 64 for d in range(4)]
        base = jnp.where(r < 64, owner[0], jnp.where(r < 128, owner[1], jnp.where(r < 192, owner[2], owner[3])))
        return (base + (r & 63)).astype(f32)

    share = []
    for h in range(2):
        at = lambda n, h=h: (ssh.at[4 * h + n], rsh.at[4 * h + n])
        share.append(
            [
                remote(shared.at[h, 0], shared.at[h, 1], *at(0), line(h, 1)),
                remote(shared.at[h, 0], shared.at[h, 2], *at(1), line(h, 3)),
                remote(shared.at[h, 1, 0:128], shared.at[h, 3, 0:128], *at(2), line(h, 1)),
                remote(shared.at[h, 2, 128:256], shared.at[h, 3, 128:256], *at(3), line(h, 3)),
            ]
        )
    for n in range(2):
        for h in range(2):
            share[h][n].start()
    for c in told:
        c.wait_recv()
    for load in loads:
        load.wait()

    def dealt(h, d, a):
        there = arrived.at[0, PLACE[d], a] if h == 0 else arrived.at[1, a, PLACE[d]]
        n = 16 * h + 4 * d + a
        return remote(outgoing.at[h, d, a], there, sd.at[n], rd.at[n], cross(h, d))

    def deal(a):
        for h in range(2):
            place = slots_of(h)
            pick = (place == told_all[h, a, 0:1, :]) | (place == told_all[h, a, 1:2, :])
            pick = jnp.where(pick, 1.0, 0.0).astype(bf16)
            for n in range(2):
                cols = slice(n * 512, n * 512 + 512)
                rows = jnp.dot(pick, shared[h, a, :, cols], preferred_element_type=f32).astype(bf16)
                if h == 0:
                    arrived[0, 0, a, :, cols] = rows[0:64]
                else:
                    arrived[1, a, 0, :, cols] = rows[0:64]
                for d in (1, 2, 3):
                    outgoing[h, d, a, :, cols] = rows[64 * d : 64 * d + 64]
        for d in (2, 1, 3):
            for h in range(2):
                dealt(h, d, a).start()

    deal(0)
    for n in range(2):
        for h in range(2):
            share[h][n].wait_recv()
            share[h][n + 2].start()
    deal(1)
    deal(2)
    for n in (2, 3):
        for h in range(2):
            share[h][n].wait_recv()
    deal(3)

    def given(h, d, a):
        zp, yp = (PLACE[d], a) if h == 0 else (a, PLACE[d])
        n = 16 * h + 4 * d + a
        return remote(result.at[h, zp, yp], returned.at[h, d, a], sg.at[n], rg.at[n], cross(h, 4 - d))

    for i, j in ((0, 0), (0, 1), (1, 0), (1, 1)):
        zs, ys = (2 * i, 2 * i + 1), (2 * j, 2 * j + 1)
        for zp in zs:
            for yp in ys:
                if zp > 0:
                    dealt(0, SHIFT[zp], yp).wait_recv()
                if yp > 0:
                    dealt(1, SHIFT[yp], zp).wait_recv()

        @pl.loop(0, 4)
        def _(n):
            cols = pl.ds(pl.multiple_of(n * 256, 256), 256)
            r0 = arrived[0, 2 * i : 2 * i + 2, 2 * j : 2 * j + 2].reshape(256, 1024)
            r1 = arrived[1, 2 * i : 2 * i + 2, 2 * j : 2 * j + 2].reshape(256, 1024)
            gate = jnp.dot(r0, wg[0:1024, cols], preferred_element_type=f32)
            gate = gate + jnp.dot(r1, wg[1024:2048, cols], preferred_element_type=f32)
            up = jnp.dot(r0, wu[0:1024, cols], preferred_element_type=f32)
            up = up + jnp.dot(r1, wu[1024:2048, cols], preferred_element_type=f32)
            hidden[:, cols] = (gate / (1.0 + jnp.exp(-gate)) * up).astype(bf16)

        for h in range(2):

            @pl.loop(0, 2)
            def _(n, h=h):
                cols = pl.ds(pl.multiple_of(n * 512, 512), 512)
                wide = pl.ds(pl.multiple_of(n * 512 + h * 1024, 512), 512)
                rows = jnp.dot(hidden[...], wd[:, wide], preferred_element_type=f32).astype(bf16)
                for p, zp in enumerate(zs):
                    for q, yp in enumerate(ys):
                        part = rows[128 * p + 64 * q : 128 * p + 64 * q + 64]
                        if h == 0 and zp == 0:
                            returned[0, 0, yp, :, cols] = part
                        elif h == 1 and yp == 0:
                            returned[1, 0, zp, :, cols] = part
                        else:
                            result[h, zp, yp, :, cols] = part

            for zp in zs:
                for yp in ys:
                    if h == 0 and zp > 0:
                        given(0, SHIFT[zp], yp).start()
                    if h == 1 and yp > 0:
                        given(1, SHIFT[yp], zp).start()

    for h in range(2):
        for c in share[h]:
            c.wait_send()

    def summed(h, a):
        n = 3 * h + a - 1
        return remote(shared.at[h, a], final.at[h, a - 1], sf.at[n], rf.at[n], line(h, 4 - SHIFT[a]))

    for a in (1, 2, 3, 0):
        for h in range(2):
            for d in (1, 2, 3):
                given(h, d, a).wait_recv()
            place = slots_of(h)
            share_of = jnp.where(place == told_all[h, a, 0:1, :], told_all[h, a, 2:3, :], 0.0)
            share_of = share_of + jnp.where(place == told_all[h, a, 1:2, :], told_all[h, a, 3:4, :], 0.0)
            share_of = share_of.T
            high = share_of.astype(bf16)
            low = (share_of - high.astype(f32)).astype(bf16)
            for n in range(2):
                cols = slice(n * 512, n * 512 + 512)
                rows = returned[h, :, a, :, cols].reshape(256, 512)
                t = jnp.dot(high, rows, preferred_element_type=f32) + jnp.dot(low, rows, preferred_element_type=f32)
                if a == 0:
                    wide = slice(h * 1024 + n * 512, h * 1024 + n * 512 + 512)
                    after[:, wide] = after[:, wide] + t
                else:
                    shared[h, a, :, cols] = t.astype(bf16)
            if a > 0:
                summed(h, a).start()
    for h in range(2):
        for a in (1, 2, 3):
            summed(h, a).wait_recv()
        wide = slice(h * 1024, h * 1024 + 1024)
        t = after[:, wide]
        for n in range(3):
            t = t + final[h, n].astype(f32)
        out[:, wide] = t.astype(bf16)
    for h in range(2):
        for a in range(4):
            for d in (1, 2, 3):
                dealt(h, d, a).wait_send()
                given(h, d, a).wait_send()
        for a in (1, 2, 3):
            summed(h, a).wait_send()
    for c in told + a1 + b1 + w1 + a2 + b2 + w2 + asks:
        c.wait_send()
    for n in range(16):

        @pl.when(lax.rem(y, 2) != n)
        def _(n=n):
            remote(attended.at[n], heads.at[:, mine], so.at[n], ro.at[me], me).wait_send()

    for g in range(4):
        for c in to_x(g) + [to_core(g, d) for d in range(4)]:
            c.wait_send()


def layer(q_slab, lat_a, lat_b, up_k, up_vt, wo, resid, gain, told, wg, wu, wd):
    v, a = pl.BlockSpec(memory_space=pltpu.VMEM), pl.BlockSpec(memory_space=pl.ANY)
    bf16, f32 = jnp.bfloat16, jnp.float32
    dma = pltpu.SemaphoreType.DMA
    return pl.pallas_call(
        layer_kernel,
        name="layer",
        out_shape=jax.ShapeDtypeStruct((256, 2048), bf16),
        in_specs=[a, a, a, v, v, a] + [v] * 3 + [a] * 3,
        out_specs=v,
        scratch_shapes=[
            pltpu.VMEM((2048, 1024), bf16),
            pltpu.VMEM((2048, 1024), bf16),
            pltpu.VMEM((1024, 2048), bf16),
            pltpu.VMEM((256, 2048), f32),
            pltpu.VMEM((2, 4, 8, 256), f32),
            pltpu.VMEM((2, 4, 256, 1024), bf16),
            pltpu.VMEM((2, 4, 4, 64, 1024), bf16),
            pltpu.VMEM((2, 4, 4, 64, 1024), bf16),
            pltpu.VMEM((256, 1024), bf16),
            pltpu.VMEM((2, 4, 4, 64, 1024), bf16),
            pltpu.VMEM((2, 4, 4, 64, 1024), bf16),
            pltpu.VMEM((2, 3, 256, 1024), bf16),
            pltpu.VMEM((16, 192, 256), bf16),
            pltpu.VMEM((4, 4, 256, 128), bf16),
            pltpu.VMEM((4, 4, 384, 128), bf16),
            pltpu.VMEM((4096, 256), bf16),
            pltpu.VMEM((144, 4096), bf16),
            pltpu.VMEM((16, 256, 128), bf16),
            pltpu.VMEM((256, 2048), bf16),
            pltpu.VMEM((8, 4, 4, 128, 256), bf16),
            dma((3,)),
        ]
        + [dma((8,))] * 4
        + [dma((32,))] * 4
        + [dma((6,))] * 2
        + [dma((4,))] * 9
        + [dma((16,))] * 4
        + [dma((4,))] * 4
        + [dma((4, 4))] * 4,
        compiler_params=pltpu.CompilerParams(
            collective_id=1, has_side_effects=True, vmem_limit_bytes=65400 * 1024
        ),
    )(q_slab, lat_a, lat_b, up_k, up_vt, wo, resid, gain, told, wg, wu, wd)


def shards(
    query_nope,
    query_rope,
    latent,
    key_rope,
    resid,
    latent_gain,
    key_up,
    value_up,
    out_proj,
    norm_gain,
    expert_gate,
    expert_up,
    expert_down,
    routes,
    route_weight,
):
    tokens = latent.shape[1]
    local_pos = lax.axis_index("sp") * tokens + jnp.arange(tokens, dtype=jnp.int32)
    latent_normed = rms_scaled(latent[0], latent_gain).astype(jnp.bfloat16)
    key_turned = rotate(key_rope[0], local_pos)
    query_turned = rotate(query_rope[0], local_pos)
    half = tokens // 2
    q_slab = jnp.concatenate(
        [query_nope[0].transpose(1, 2, 0), query_turned.transpose(1, 2, 0)], axis=1
    )
    key_pack = jnp.concatenate([key_turned[:half], key_turned[half:]], axis=1)
    lat_a = latent_normed[:, :128]
    lat_b = jnp.concatenate([latent_normed[:, 128:], key_pack], axis=0)
    told = jnp.concatenate(
        [routes[0].T.astype(jnp.float32), route_weight[0].T, jnp.zeros((4, tokens), jnp.float32)], axis=0
    )
    return layer(
        q_slab, lat_a, lat_b, key_up, value_up.T, out_proj, resid[0], norm_gain[None], told,
        expert_gate[0], expert_up[0], expert_down[0],
    )[None]


def solution(mesh):
    return jax.shard_map(
        shards,
        mesh=mesh,
        in_specs=(
            P("dp", "sp", None, None),
            P("dp", "sp", None, None),
            P("dp", "sp", None),
            P("dp", "sp", None),
            P("dp", "sp", None),
            P(),
            P(None, "sp"),
            P(None, "sp"),
            P("sp", "dp"),
            P(),
            P("sp", None, None),
            P("sp", None, None),
            P("sp", None, None),
            P("dp", "sp", None),
            P("dp", "sp", None),
        ),
        out_specs=P("dp", "sp", None),
        check_vma=False,
    )
```

```python
import math

import jax
import jax.numpy as jnp
from jax import lax
from jax.experimental import pallas as pl
from jax.experimental.pallas import tpu as pltpu
from jax.sharding import PartitionSpec as P

epsilon = 1e-06
rope_base = 10000.0
masked_score = -1e30


ORDER = [(0, 0), (2, 2), (3, 2), (2, 3), (1, 2), (2, 1), (0, 2), (2, 0), (3, 1), (1, 3), (3, 3), (1, 1), (3, 0), (0, 3), (1, 0), (0, 1)]
MESH = pl.DeviceIdType.MESH


def packed(digits):
    value = sum(d << (2 * i) for i, d in enumerate(digits))
    return value - (1 << 32) if value >= 1 << 31 else value


PLACE = {0: 0, 1: 1, 3: 2, 2: 3}
EARLY = 3
SHIFT = [0, 1, 3, 2]
PAIRS = [(0, 0), (2, 1), (1, 1), (3, 1), (2, 0), (0, 1), (1, 0), (3, 0)]
PZ, PJ = packed([o[0] for o in PAIRS]), packed([o[1] for o in PAIRS])


def shifted(me, dz, dy):
    z, y = me // 4, lax.rem(me, 4)
    return lax.rem(z + dz, 4) * 4 + lax.rem(y + dy, 4)


def remote(src, dst, send, recv, target):
    return pltpu.make_async_remote_copy(
        src_ref=src,
        dst_ref=dst,
        send_sem=send,
        recv_sem=recv,
        device_id={"sp": target},
        device_id_type=MESH,
    )


def layer_kernel(
    nope_t, rope_t, lat_in, lat_gain, key_t, cosine, sine, up_k, up_v, wo_hbm, resid, gain, routes_t, weight_t, wg_hbm, wu_hbm, wd_hbm, out,
    wg, wu, wd, told_all, shared, outgoing, arrived, hidden, result, returned, final,
    q_out, q_in, la, lb, up_vt, keys, vals, attended, heads, wo,
    wsem, st, rt, ssh, rsh, sd, rd, sg, rg, sf, rf,
    lsem, sa1, ra1, sb1, rb1, sa2, ra2, sb2, rb2, sq, rq, so, ro, swz, rwz, swy, rwy, swx, rwx, swc, rwc,
):
    me, dp = lax.axis_index("sp"), lax.axis_index("dp")
    z, y = me // 4, lax.rem(me, 4)
    x, core = dp // 2, lax.rem(dp, 2)
    f32, bf16, i32 = jnp.float32, jnp.bfloat16, jnp.int32
    barrier = pltpu.get_barrier_semaphore()
    for dz, dy in ORDER[1:]:
        pl.semaphore_signal(barrier, inc=1, device_id={"sp": shifted(me, dz, dy)}, device_id_type=MESH)
    x_peer = [None] + [lax.rem(x + d, 4) * 2 + core for d in (1, 2, 3)]
    x_from = [dp] + [lax.rem(x + 4 - d, 4) * 2 + core for d in (1, 2, 3)]
    other = x * 2 + 1 - core
    for t in x_peer[1:] + [other]:
        pl.semaphore_signal(barrier, inc=1, device_id={"dp": t}, device_id_type=MESH)
    fill_wo = pltpu.make_async_copy(wo_hbm, wo.at[dp, z, y], lsem.at[0])
    fill_wo.start()
    loads = [
        pltpu.make_async_copy(a, b, wsem.at[i])
        for i, (a, b) in enumerate(((wg_hbm, wg), (wu_hbm, wu), (wd_hbm, wd)))
    ]
    for load in loads:
        load.start()
    tok = lax.broadcasted_iota(i32, (256, 256), 0)
    tok_l = lax.broadcasted_iota(i32, (256, 256), 1)
    upper = jnp.where(tok < tok_l, 1.0, 0.0).astype(bf16)
    expert = lax.broadcasted_iota(i32, (16, 256), 0).astype(f32)
    hot = [jnp.where(expert == routes_t[k : k + 1, :].astype(f32), 1.0, 0.0) for k in range(2)]
    before = jnp.dot((hot[0] + hot[1]).astype(bf16), upper, preferred_element_type=f32) + expert * 64.0
    for h in range(2):
        for k in range(2):
            told_all[h, 0, k : k + 1, :] = jnp.sum(hot[k] * before, axis=0, keepdims=True)
        told_all[h, 0, 2:4, :] = weight_t[...]
        told_all[h, 0, 4:8, :] = jnp.zeros((4, 256), f32)

    lat = lat_in[...].astype(f32)
    lat = lat * lax.rsqrt(jnp.mean(lat * lat, axis=-1, keepdims=True) + epsilon) * lat_gain[...]
    la[z, y] = lat[:, 0:128].astype(bf16)
    lb[z, y, 0:256, :] = lat[:, 128:256].astype(bf16)
    cos, sin = cosine[...], sine[...]
    a, b = key_t[0:32, :].astype(f32), key_t[32:64, :].astype(f32)
    turned = jnp.concatenate([a * cos - b * sin, b * cos + a * sin], axis=0)
    lb[z, y, 256:384, :] = jnp.concatenate([turned[:, 0:128], turned[:, 128:256]], axis=0).T.astype(bf16)
    up_vt[...] = up_v[...].astype(f32).T.astype(bf16)

    @pl.loop(0, 16)
    def _(h):
        a, b = rope_t[h, 0:32, :].astype(f32), rope_t[h, 32:64, :].astype(f32)
        q_out[h, 0:128, :] = nope_t[h]
        q_out[h, 128:160, :] = (a * cosine[...] - b * sine[...]).astype(bf16)
        q_out[h, 160:192, :] = (b * cosine[...] + a * sine[...]).astype(bf16)

    q_in[me] = q_out[me]
    fill_wo.wait()
    pl.semaphore_wait(barrier, 19)

    def along(dz, dy):
        return shifted(me, dz, dy)

    told = []
    for h in range(2):
        for d in (1, 2, 3):
            target = along(0, d) if h == 0 else along(d, 0)
            told.append(remote(told_all.at[h, 0], told_all.at[h, PLACE[d]], st.at[4 * h + d], rt.at[4 * h + d], target))
    a1 = [remote(la.at[z, y], la.at[z, y], sa1.at[d], ra1.at[d], along(d, 0)) for d in (1, 2, 3)]
    b1 = [remote(lb.at[z, y], lb.at[z, y], sb1.at[d], rb1.at[d], along(0, d)) for d in (1, 2, 3)]
    w1 = [remote(wo.at[dp, z, y], wo.at[dp, z, y], swz.at[d], rwz.at[d], along(d, 0)) for d in (1, 2, 3)]
    ym, yp, yo = [lax.rem(y + n, 4) for n in (3, 1, 2)]
    zm, zp, zo = [lax.rem(z + n, 4) for n in (3, 1, 2)]
    up, down, fore, back = along(0, 1), along(0, 3), along(1, 0), along(3, 0)
    a2 = [
        remote(la.at[:, y], la.at[:, y], sa2.at[0], ra2.at[0], up),
        remote(la.at[:, y], la.at[:, y], sa2.at[1], ra2.at[1], down),
        remote(la.at[0:2, ym], la.at[0:2, ym], sa2.at[2], ra2.at[2], up),
        remote(la.at[2:4, yp], la.at[2:4, yp], sa2.at[3], ra2.at[3], down),
    ]
    b2 = [
        remote(lb.at[z], lb.at[z], sb2.at[0], rb2.at[0], fore),
        remote(lb.at[z], lb.at[z], sb2.at[1], rb2.at[1], back),
        remote(lb.at[zm, 0:2], lb.at[zm, 0:2], sb2.at[2], rb2.at[2], fore),
        remote(lb.at[zp, 2:4], lb.at[zp, 2:4], sb2.at[3], rb2.at[3], back),
    ]
    w2 = [
        remote(wo.at[dp, :, y], wo.at[dp, :, y], swy.at[0], rwy.at[0], up),
        remote(wo.at[dp, :, y], wo.at[dp, :, y], swy.at[1], rwy.at[1], down),
        remote(wo.at[dp, 0:2, ym], wo.at[dp, 0:2, ym], swy.at[2], rwy.at[2], up),
        remote(wo.at[dp, 2:4, yp], wo.at[dp, 2:4, yp], swy.at[3], rwy.at[3], down),
    ]
    asks = []
    for r, (dz, dj) in enumerate(PAIRS):
        for e in range(2):
            if r == 0:
                target = me + 1 - 2 * lax.rem(y, 2)
                if e == 1:
                    continue
            else:
                target = lax.rem(z + 4 - dz, 4) * 4 + lax.rem(y // 2 + dj, 2) * 2 + e
            asks.append(remote(q_out.at[target], q_in.at[me], sq.at[2 * r + e], rq.at[me], target))

    def to_x(g):
        part = wo.at[dp, :, lax.rem(y + 4 - g, 4)]
        copies = [
            pltpu.make_async_remote_copy(
                src_ref=part, dst_ref=part, send_sem=swx.at[g, d], recv_sem=rwx.at[g, d],
                device_id={"dp": x_peer[d]}, device_id_type=MESH,
            )
            for d in (1, 2, 3)
        ]
        return copies

    def to_core(g, d):
        part = wo.at[x_from[d], :, lax.rem(y + 4 - g, 4)]
        return pltpu.make_async_remote_copy(
            src_ref=part, dst_ref=part, send_sem=swc.at[g, d], recv_sem=rwc.at[g, d],
            device_id={"dp": other}, device_id_type=MESH,
        )

    for c in w1 + a1 + b1:
        c.start()
    for c in w1:
        c.wait_recv()
    for c in to_x(0) + [to_core(0, 0)]:
        c.start()
    for c in a1:
        c.wait_recv()
    for c in a2[:2]:
        c.start()
    for c in b1:
        c.wait_recv()
    for c in b2[:2] + w2[:2] + told + asks[:EARLY]:
        c.start()
    vals[128:144, :] = jnp.ones((16, 4096), bf16)

    def build(bz, by):
        b = bz * 4 + by
        start = pl.multiple_of(b * 256, 256)
        rows = pl.ds(start, 256)
        lat = jnp.concatenate([la[bz, by], lb[bz, by, 0:256, :]], axis=1)
        keys[rows, 0:128] = jnp.dot(lat, up_k[...], preferred_element_type=f32).astype(bf16)
        vals[0:128, rows] = lax.dot_general(
            up_vt[...], lat, (((1,), (1,)), ((), ())), preferred_element_type=f32
        ).astype(bf16)
        turn = lb[bz, by, 256:384, :].astype(f32)
        keys[pl.ds(start, 128), 128:256] = turn.astype(bf16)
        keys[pl.ds(pl.multiple_of(start + 128, 128), 128), 128:256] = pltpu.roll(turn, 64, 1).astype(bf16)

    for n in range(2):
        a2[n].wait_recv()
        a2[n + 2].start()
    for n in range(2):
        b2[n].wait_recv()
        b2[n + 2].start()
    for n in range(2):
        w2[n].wait_recv()
        w2[n + 2].start()
        for c in to_x(2 * n + 1) + [to_core(2 * n + 1, 0)]:
            c.start()
    for c in asks[EARLY:]:
        c.start()

    @pl.loop(0, 9)
    def _(n):
        build(lax.rem(z + 3 + n // 3, 4), lax.rem(y + 3 + lax.rem(n, 3), 4))

    for c in a2[2:] + b2[2:]:
        c.wait_recv()

    @pl.loop(0, 4)
    def _(n):
        build(zo, lax.rem(y + n, 4))

    @pl.loop(0, 3)
    def _(n):
        build(lax.rem(z + 3 + n, 4), yo)

    for c in w2[2:]:
        c.wait_recv()
    for c in to_x(2) + [to_core(2, 0)]:
        c.start()
    unit = 192.0 ** -0.5 * math.log2(math.e)
    mine = pl.ds(pl.multiple_of(me * 128, 128), 128)

    def one_pair(r, _):
        dz, dj = (PZ >> (2 * r)) & 3, (PJ >> (2 * r)) & 3
        pair = lax.rem(z + dz, 4) * 2 + lax.rem(y // 2 + dj, 2)
        for e in range(2):
            source = 2 * pair + e

            @pl.when(source != me)
            def _(source=source):
                remote(q_in.at[source], q_in.at[source], sq.at[0], rq.at[source], source).wait_recv()

        for i, g in enumerate((0, 1, 3)):

            @pl.when(r == 2 * i + 2)
            def _(g=g):
                for d in (1, 2, 3):
                    to_x(g)[d - 1].wait_recv()
                    to_core(g, d).start()

        q = jnp.concatenate([q_in[2 * pair], q_in[2 * pair + 1]], axis=1)

        def scores(at):
            return jnp.dot(keys[pl.ds(at, 512), 0:192], q, preferred_element_type=f32)

        def weigh(s, at, top, acc):
            new = jnp.maximum(top, jnp.max(s, axis=0, keepdims=True) * unit)
            p = jnp.exp2(s * unit - new).astype(bf16)
            return new, acc * jnp.exp2(top - new) + jnp.dot(
                vals[:, pl.ds(at, 512)], p, preferred_element_type=f32
            )

        last = pl.multiple_of(pair * 512, 512)
        key_id = lax.broadcasted_iota(i32, (512, 512), 0)
        row_id = lax.broadcasted_iota(i32, (512, 512), 1)
        s = jnp.where(key_id <= row_id, scores(last), masked_score)
        top = jnp.max(s, axis=0, keepdims=True) * unit
        p = jnp.exp2(s * unit - top).astype(bf16)
        acc = jnp.dot(vals[:, pl.ds(last, 512)], p, preferred_element_type=f32)

        def single(i, carry):
            at = pl.multiple_of((pair - 1) * 512, 512)
            return weigh(scores(at), at, *carry)

        def double(i, carry):
            at = pl.multiple_of(i * 1024, 1024)
            then = pl.multiple_of(at + 512, 512)
            s, t = scores(at), scores(then)
            return weigh(t, then, *weigh(s, at, *carry))

        carry = lax.fori_loop(0, lax.rem(pair, 2), single, (top, acc))
        top, acc = lax.fori_loop(0, pair // 2, double, carry)
        rows = acc[0:128] / acc[128:129]
        for e in range(2):
            attended[2 * r + e] = rows[:, 256 * e : 256 * e + 256].T.astype(bf16)
        for e in range(2):
            source = 2 * pair + e

            @pl.when(source != me)
            def _(e=e, source=source):
                remote(attended.at[2 * r + e], heads.at[:, mine], so.at[2 * r + e], ro.at[me], source).start()

            @pl.when(source == me)
            def _(e=e):
                heads[:, mine] = attended[2 * r + e]

        return 0

    lax.fori_loop(0, 8, one_pair, 0)
    for d in (1, 2, 3):
        to_x(2)[d - 1].wait_recv()
        to_core(2, d).start()
    for k in range(1, 16):
        head = along(*ORDER[k])
        there = pl.ds(pl.multiple_of(head * 128, 128), 128)
        remote(attended.at[0], heads.at[:, there], so.at[0], ro.at[head], head).wait_recv()
    for g in range(4):
        for d in range(4):
            to_core(g, d).wait_recv()

    @pl.loop(0, 8)
    def _(n):
        cols = pl.ds(pl.multiple_of(n * 256, 256), 256)
        p = jnp.dot(heads[...], wo[n].reshape(2048, 256), preferred_element_type=f32).astype(bf16)
        out[:, cols] = resid[:, cols].astype(f32) + p.astype(f32)

    @pl.loop(0, 8)
    def _(r):
        rows = pl.ds(pl.multiple_of(r * 32, 32), 32)
        a = out[rows, :]
        scale = lax.rsqrt(jnp.mean(a * a, axis=-1, keepdims=True) + epsilon)
        full = (a * scale * gain[...]).astype(bf16)
        shared[0, 0, rows, :] = full[:, 0:1024]
        shared[1, 0, rows, :] = full[:, 1024:2048]

    def line(h, d):
        return along(0, d) if h == 0 else along(d, 0)

    def cross(h, d):
        return along(d, 0) if h == 0 else along(0, d)

    def slots_of(h):
        r = lax.broadcasted_iota(i32, (256, 1), 0)
        owner = [cross(h, d) * 64 for d in range(4)]
        base = jnp.where(r < 64, owner[0], jnp.where(r < 128, owner[1], jnp.where(r < 192, owner[2], owner[3])))
        return (base + (r & 63)).astype(f32)

    share = []
    for h in range(2):
        at = lambda n, h=h: (ssh.at[4 * h + n], rsh.at[4 * h + n])
        share.append(
            [
                remote(shared.at[h, 0], shared.at[h, 1], *at(0), line(h, 1)),
                remote(shared.at[h, 0], shared.at[h, 2], *at(1), line(h, 3)),
                remote(shared.at[h, 1, 0:128], shared.at[h, 3, 0:128], *at(2), line(h, 1)),
                remote(shared.at[h, 2, 128:256], shared.at[h, 3, 128:256], *at(3), line(h, 3)),
            ]
        )
    for n in range(2):
        for h in range(2):
            share[h][n].start()
    for c in told:
        c.wait_recv()
    for load in loads:
        load.wait()

    def dealt(h, d, a):
        there = arrived.at[0, PLACE[d], a] if h == 0 else arrived.at[1, a, PLACE[d]]
        n = 16 * h + 4 * d + a
        return remote(outgoing.at[h, d, a], there, sd.at[n], rd.at[n], cross(h, d))

    def deal(a):
        for h in range(2):
            place = slots_of(h)
            pick = (place == told_all[h, a, 0:1, :]) | (place == told_all[h, a, 1:2, :])
            pick = jnp.where(pick, 1.0, 0.0).astype(bf16)
            for n in range(2):
                cols = slice(n * 512, n * 512 + 512)
                rows = jnp.dot(pick, shared[h, a, :, cols], preferred_element_type=f32).astype(bf16)
                if h == 0:
                    arrived[0, 0, a, :, cols] = rows[0:64]
                else:
                    arrived[1, a, 0, :, cols] = rows[0:64]
                for d in (1, 2, 3):
                    outgoing[h, d, a, :, cols] = rows[64 * d : 64 * d + 64]
        for d in (2, 1, 3):
            for h in range(2):
                dealt(h, d, a).start()

    deal(0)
    for n in range(2):
        for h in range(2):
            share[h][n].wait_recv()
            share[h][n + 2].start()
    deal(1)
    deal(2)
    for n in (2, 3):
        for h in range(2):
            share[h][n].wait_recv()
    deal(3)

    def given(h, d, a):
        zp, yp = (PLACE[d], a) if h == 0 else (a, PLACE[d])
        n = 16 * h + 4 * d + a
        return remote(result.at[h, zp, yp], returned.at[h, d, a], sg.at[n], rg.at[n], cross(h, 4 - d))

    for i, j in ((0, 0), (0, 1), (1, 0), (1, 1)):
        zs, ys = (2 * i, 2 * i + 1), (2 * j, 2 * j + 1)
        for zp in zs:
            for yp in ys:
                if zp > 0:
                    dealt(0, SHIFT[zp], yp).wait_recv()
                if yp > 0:
                    dealt(1, SHIFT[yp], zp).wait_recv()

        @pl.loop(0, 4)
        def _(n):
            cols = pl.ds(pl.multiple_of(n * 256, 256), 256)
            r0 = arrived[0, 2 * i : 2 * i + 2, 2 * j : 2 * j + 2].reshape(256, 1024)
            r1 = arrived[1, 2 * i : 2 * i + 2, 2 * j : 2 * j + 2].reshape(256, 1024)
            gate = jnp.dot(r0, wg[0:1024, cols], preferred_element_type=f32)
            gate = gate + jnp.dot(r1, wg[1024:2048, cols], preferred_element_type=f32)
            up = jnp.dot(r0, wu[0:1024, cols], preferred_element_type=f32)
            up = up + jnp.dot(r1, wu[1024:2048, cols], preferred_element_type=f32)
            hidden[:, cols] = (gate / (1.0 + jnp.exp(-gate)) * up).astype(bf16)

        for h in range(2):

            @pl.loop(0, 2)
            def _(n, h=h):
                cols = pl.ds(pl.multiple_of(n * 512, 512), 512)
                wide = pl.ds(pl.multiple_of(n * 512 + h * 1024, 512), 512)
                rows = jnp.dot(hidden[...], wd[:, wide], preferred_element_type=f32).astype(bf16)
                for p, zp in enumerate(zs):
                    for q, yp in enumerate(ys):
                        part = rows[128 * p + 64 * q : 128 * p + 64 * q + 64]
                        if h == 0 and zp == 0:
                            returned[0, 0, yp, :, cols] = part
                        elif h == 1 and yp == 0:
                            returned[1, 0, zp, :, cols] = part
                        else:
                            result[h, zp, yp, :, cols] = part

            for zp in zs:
                for yp in ys:
                    if h == 0 and zp > 0:
                        given(0, SHIFT[zp], yp).start()
                    if h == 1 and yp > 0:
                        given(1, SHIFT[yp], zp).start()

    for h in range(2):
        for c in share[h]:
            c.wait_send()

    def summed(h, a):
        n = 3 * h + a - 1
        return remote(shared.at[h, a], final.at[h, a - 1], sf.at[n], rf.at[n], line(h, 4 - SHIFT[a]))

    for a in (1, 2, 3, 0):
        for h in range(2):
            for d in (1, 2, 3):
                given(h, d, a).wait_recv()
            place = slots_of(h)
            share_of = jnp.where(place == told_all[h, a, 0:1, :], told_all[h, a, 2:3, :], 0.0)
            share_of = share_of + jnp.where(place == told_all[h, a, 1:2, :], told_all[h, a, 3:4, :], 0.0)
            share_of = share_of.T
            high = share_of.astype(bf16)
            low = (share_of - high.astype(f32)).astype(bf16)
            for n in range(2):
                cols = slice(n * 512, n * 512 + 512)
                rows = returned[h, :, a, :, cols].reshape(256, 512)
                t = jnp.dot(high, rows, preferred_element_type=f32) + jnp.dot(low, rows, preferred_element_type=f32)
                if a == 0:
                    wide = slice(h * 1024 + n * 512, h * 1024 + n * 512 + 512)
                    out[:, wide] = out[:, wide] + t
                else:
                    shared[h, a, :, cols] = t.astype(bf16)
            if a > 0:
                summed(h, a).start()
    for h in range(2):
        for a in (1, 2, 3):
            summed(h, a).wait_recv()
        wide = slice(h * 1024, h * 1024 + 1024)
        t = out[:, wide]
        for n in range(3):
            t = t + final[h, n].astype(f32)
        out[:, wide] = t
    for h in range(2):
        for a in range(4):
            for d in (1, 2, 3):
                dealt(h, d, a).wait_send()
                given(h, d, a).wait_send()
        for a in (1, 2, 3):
            summed(h, a).wait_send()
    for c in told + a1 + b1 + w1 + a2 + b2 + w2 + asks:
        c.wait_send()
    for n in range(16):

        @pl.when(lax.rem(y, 2) != n)
        def _(n=n):
            remote(attended.at[n], heads.at[:, mine], so.at[n], ro.at[me], me).wait_send()

    for g in range(4):
        for c in to_x(g) + [to_core(g, d) for d in range(4)]:
            c.wait_send()


def layer(nope_t, rope_t, lat, lat_gain, key_t, cos, sin, up_k, up_v, wo, resid, gain, routes_t, weight_t, wg, wu, wd):
    v, a = pl.BlockSpec(memory_space=pltpu.VMEM), pl.BlockSpec(memory_space=pl.ANY)
    bf16, f32 = jnp.bfloat16, jnp.float32
    dma = pltpu.SemaphoreType.DMA
    return pl.pallas_call(
        layer_kernel,
        name="layer",
        out_shape=jax.ShapeDtypeStruct((256, 2048), f32),
        in_specs=[v] * 9 + [a] + [v] * 4 + [a] * 3,
        out_specs=v,
        scratch_shapes=[
            pltpu.VMEM((2048, 1024), bf16),
            pltpu.VMEM((2048, 1024), bf16),
            pltpu.VMEM((1024, 2048), bf16),
            pltpu.VMEM((2, 4, 8, 256), f32),
            pltpu.VMEM((2, 4, 256, 1024), bf16),
            pltpu.VMEM((2, 4, 4, 64, 1024), bf16),
            pltpu.VMEM((2, 4, 4, 64, 1024), bf16),
            pltpu.VMEM((256, 1024), bf16),
            pltpu.VMEM((2, 4, 4, 64, 1024), bf16),
            pltpu.VMEM((2, 4, 4, 64, 1024), bf16),
            pltpu.VMEM((2, 3, 256, 1024), bf16),
            pltpu.VMEM((16, 192, 256), bf16),
            pltpu.VMEM((16, 192, 256), bf16),
            pltpu.VMEM((4, 4, 256, 128), bf16),
            pltpu.VMEM((4, 4, 384, 128), bf16),
            pltpu.VMEM((128, 256), bf16),
            pltpu.VMEM((4096, 256), bf16),
            pltpu.VMEM((144, 4096), bf16),
            pltpu.VMEM((16, 256, 128), bf16),
            pltpu.VMEM((256, 2048), bf16),
            pltpu.VMEM((8, 4, 4, 128, 256), bf16),
            dma((3,)),
        ]
        + [dma((8,))] * 4
        + [dma((32,))] * 4
        + [dma((6,))] * 2
        + [dma((4,))] * 9
        + [dma((16,))] * 4
        + [dma((4,))] * 4
        + [dma((4, 4))] * 4,
        compiler_params=pltpu.CompilerParams(
            collective_id=1, has_side_effects=True, vmem_limit_bytes=65400 * 1024
        ),
    )(nope_t, rope_t, lat, lat_gain, key_t, cos, sin, up_k, up_v, wo, resid, gain, routes_t, weight_t, wg, wu, wd)


def shards(
    query_nope,
    query_rope,
    latent,
    key_rope,
    resid,
    latent_gain,
    key_up,
    value_up,
    out_proj,
    norm_gain,
    expert_gate,
    expert_up,
    expert_down,
    routes,
    route_weight,
):
    tokens = latent.shape[1]
    positions = lax.axis_index("sp") * tokens + jnp.arange(tokens, dtype=jnp.int32)
    half_width = key_rope.shape[-1] // 2
    frequency = rope_base ** (-jnp.arange(half_width, dtype=jnp.float32) / half_width)
    angles = frequency[:, None] * positions.astype(jnp.float32)[None, :]
    return layer(
        query_nope[0].transpose(1, 2, 0), query_rope[0].transpose(1, 2, 0), latent[0], latent_gain[None],
        key_rope[0].T, jnp.cos(angles), jnp.sin(angles), key_up, value_up, out_proj, resid[0], norm_gain[None],
        routes[0].T, route_weight[0].T, expert_gate[0], expert_up[0], expert_down[0],
    ).astype(jnp.bfloat16)[None]


def solution(mesh):
    return jax.shard_map(
        shards,
        mesh=mesh,
        in_specs=(
            P("dp", "sp", None, None),
            P("dp", "sp", None, None),
            P("dp", "sp", None),
            P("dp", "sp", None),
            P("dp", "sp", None),
            P(),
            P(None, "sp"),
            P(None, "sp"),
            P("sp", "dp"),
            P(),
            P("sp", None, None),
            P("sp", None, None),
            P("sp", None, None),
            P("dp", "sp", None),
            P("dp", "sp", None),
        ),
        out_specs=P("dp", "sp", None),
        check_vma=False,
    )
```

```python
import math

import jax
import jax.numpy as jnp
from jax import lax
from jax.experimental import pallas as pl
from jax.experimental.pallas import tpu as pltpu
from jax.sharding import PartitionSpec as P

epsilon = 1e-06
rope_base = 10000.0
masked_score = -1e30


ORDER = [(0, 0), (2, 2), (3, 2), (2, 3), (1, 2), (2, 1), (0, 2), (2, 0), (3, 1), (1, 3), (3, 3), (1, 1), (3, 0), (0, 3), (1, 0), (0, 1)]
MESH = pl.DeviceIdType.MESH


def packed(digits):
    value = sum(d << (2 * i) for i, d in enumerate(digits))
    return value - (1 << 32) if value >= 1 << 31 else value


PLACE = {0: 0, 1: 1, 3: 2, 2: 3}
EARLY = 3
SHIFT = [0, 1, 3, 2]
PAIRS = [(0, 0), (2, 1), (1, 1), (3, 1), (2, 0), (0, 1), (1, 0), (3, 0)]
PZ, PJ = packed([o[0] for o in PAIRS]), packed([o[1] for o in PAIRS])


def shifted(me, dz, dy):
    z, y = me // 4, lax.rem(me, 4)
    return lax.rem(z + dz, 4) * 4 + lax.rem(y + dy, 4)


def remote(src, dst, send, recv, target):
    return pltpu.make_async_remote_copy(
        src_ref=src,
        dst_ref=dst,
        send_sem=send,
        recv_sem=recv,
        device_id={"sp": target},
        device_id_type=MESH,
    )


def layer_kernel(
    nope, rope_t, lat_in, lat_gain, key_t, cosine, sine, up_k, up_v, wo_hbm, resid, gain, routes_t, weight_t, wg_hbm, wu_hbm, wd_hbm, out,
    wg, wu, wd, told_all, shared, outgoing, arrived, hidden, result, returned, final,
    q_out, q_in, la, lb, up_vt, keys, vals, attended, heads, wo,
    wsem, st, rt, ssh, rsh, sd, rd, sg, rg, sf, rf,
    lsem, sa1, ra1, sb1, rb1, sa2, ra2, sb2, rb2, sq, rq, so, ro, swz, rwz, swy, rwy, swx, rwx, swc, rwc,
):
    me, dp = lax.axis_index("sp"), lax.axis_index("dp")
    z, y = me // 4, lax.rem(me, 4)
    x, core = dp // 2, lax.rem(dp, 2)
    f32, bf16, i32 = jnp.float32, jnp.bfloat16, jnp.int32
    barrier = pltpu.get_barrier_semaphore()
    for dz, dy in ORDER[1:]:
        pl.semaphore_signal(barrier, inc=1, device_id={"sp": shifted(me, dz, dy)}, device_id_type=MESH)
    x_peer = [None] + [lax.rem(x + d, 4) * 2 + core for d in (1, 2, 3)]
    x_from = [dp] + [lax.rem(x + 4 - d, 4) * 2 + core for d in (1, 2, 3)]
    other = x * 2 + 1 - core
    for t in x_peer[1:] + [other]:
        pl.semaphore_signal(barrier, inc=1, device_id={"dp": t}, device_id_type=MESH)
    fill_wo = pltpu.make_async_copy(wo_hbm, wo.at[dp, z, y], lsem.at[0])
    fill_wo.start()
    loads = [
        pltpu.make_async_copy(a, b, wsem.at[i])
        for i, (a, b) in enumerate(((wg_hbm, wg), (wu_hbm, wu), (wd_hbm, wd)))
    ]
    for load in loads:
        load.start()
    tok = lax.broadcasted_iota(i32, (256, 256), 0)
    tok_l = lax.broadcasted_iota(i32, (256, 256), 1)
    upper = jnp.where(tok < tok_l, 1.0, 0.0).astype(bf16)
    expert = lax.broadcasted_iota(i32, (16, 256), 0).astype(f32)
    hot = [jnp.where(expert == routes_t[k : k + 1, :].astype(f32), 1.0, 0.0) for k in range(2)]
    before = jnp.dot((hot[0] + hot[1]).astype(bf16), upper, preferred_element_type=f32) + expert * 64.0
    for h in range(2):
        for k in range(2):
            told_all[h, 0, k : k + 1, :] = jnp.sum(hot[k] * before, axis=0, keepdims=True)
        told_all[h, 0, 2:4, :] = weight_t[...]
        told_all[h, 0, 4:8, :] = jnp.zeros((4, 256), f32)

    lat = lat_in[...].astype(f32)
    lat = lat * lax.rsqrt(jnp.mean(lat * lat, axis=-1, keepdims=True) + epsilon) * lat_gain[...]
    la[z, y] = lat[:, 0:128].astype(bf16)
    lb[z, y, 0:256, :] = lat[:, 128:256].astype(bf16)
    cos, sin = cosine[...], sine[...]
    a, b = key_t[0:32, :].astype(f32), key_t[32:64, :].astype(f32)
    turned = jnp.concatenate([a * cos - b * sin, b * cos + a * sin], axis=0)
    lb[z, y, 256:384, :] = jnp.concatenate([turned[:, 0:128], turned[:, 128:256]], axis=0).T.astype(bf16)
    up_vt[...] = up_v[...].astype(f32).T.astype(bf16)

    fill_wo.wait()
    pl.semaphore_wait(barrier, 19)

    def along(dz, dy):
        return shifted(me, dz, dy)

    told = []
    for h in range(2):
        for d in (1, 2, 3):
            target = along(0, d) if h == 0 else along(d, 0)
            told.append(remote(told_all.at[h, 0], told_all.at[h, PLACE[d]], st.at[4 * h + d], rt.at[4 * h + d], target))
    a1 = [remote(la.at[z, y], la.at[z, y], sa1.at[d], ra1.at[d], along(d, 0)) for d in (1, 2, 3)]
    b1 = [remote(lb.at[z, y], lb.at[z, y], sb1.at[d], rb1.at[d], along(0, d)) for d in (1, 2, 3)]
    w1 = [remote(wo.at[dp, z, y], wo.at[dp, z, y], swz.at[d], rwz.at[d], along(d, 0)) for d in (1, 2, 3)]
    ym, yp, yo = [lax.rem(y + n, 4) for n in (3, 1, 2)]
    zm, zp, zo = [lax.rem(z + n, 4) for n in (3, 1, 2)]
    up, down, fore, back = along(0, 1), along(0, 3), along(1, 0), along(3, 0)
    a2 = [
        remote(la.at[:, y], la.at[:, y], sa2.at[0], ra2.at[0], up),
        remote(la.at[:, y], la.at[:, y], sa2.at[1], ra2.at[1], down),
        remote(la.at[0:2, ym], la.at[0:2, ym], sa2.at[2], ra2.at[2], up),
        remote(la.at[2:4, yp], la.at[2:4, yp], sa2.at[3], ra2.at[3], down),
    ]
    b2 = [
        remote(lb.at[z], lb.at[z], sb2.at[0], rb2.at[0], fore),
        remote(lb.at[z], lb.at[z], sb2.at[1], rb2.at[1], back),
        remote(lb.at[zm, 0:2], lb.at[zm, 0:2], sb2.at[2], rb2.at[2], fore),
        remote(lb.at[zp, 2:4], lb.at[zp, 2:4], sb2.at[3], rb2.at[3], back),
    ]
    w2 = [
        remote(wo.at[dp, :, y], wo.at[dp, :, y], swy.at[0], rwy.at[0], up),
        remote(wo.at[dp, :, y], wo.at[dp, :, y], swy.at[1], rwy.at[1], down),
        remote(wo.at[dp, 0:2, ym], wo.at[dp, 0:2, ym], swy.at[2], rwy.at[2], up),
        remote(wo.at[dp, 2:4, yp], wo.at[dp, 2:4, yp], swy.at[3], rwy.at[3], down),
    ]
    asks = []
    for r, (dz, dj) in enumerate(PAIRS):
        for e in range(2):
            if r == 0:
                target = me + 1 - 2 * lax.rem(y, 2)
                if e == 1:
                    continue
            else:
                target = lax.rem(z + 4 - dz, 4) * 4 + lax.rem(y // 2 + dj, 2) * 2 + e
            asks.append(remote(q_out.at[target], q_in.at[me], sq.at[2 * r + e], rq.at[me], target))

    def to_x(g):
        part = wo.at[dp, :, lax.rem(y + 4 - g, 4)]
        copies = [
            pltpu.make_async_remote_copy(
                src_ref=part, dst_ref=part, send_sem=swx.at[g, d], recv_sem=rwx.at[g, d],
                device_id={"dp": x_peer[d]}, device_id_type=MESH,
            )
            for d in (1, 2, 3)
        ]
        return copies

    def to_core(g, d):
        part = wo.at[x_from[d], :, lax.rem(y + 4 - g, 4)]
        return pltpu.make_async_remote_copy(
            src_ref=part, dst_ref=part, send_sem=swc.at[g, d], recv_sem=rwc.at[g, d],
            device_id={"dp": other}, device_id_type=MESH,
        )

    for c in w1 + a1 + b1:
        c.start()
    for t in (0, 128):
        by_head = nope[t : t + 128].astype(f32).transpose(1, 0, 2)
        for h in range(16):
            q_out[h, 0:128, t : t + 128] = by_head[h].T.astype(bf16)

    @pl.loop(0, 16)
    def _(h):
        a, b = rope_t[h, 0:32, :].astype(f32), rope_t[h, 32:64, :].astype(f32)
        q_out[h, 128:160, :] = (a * cosine[...] - b * sine[...]).astype(bf16)
        q_out[h, 160:192, :] = (b * cosine[...] + a * sine[...]).astype(bf16)

    q_in[me] = q_out[me]
    for c in w1:
        c.wait_recv()
    for c in to_x(0) + [to_core(0, 0)]:
        c.start()
    for c in a1:
        c.wait_recv()
    for c in a2[:2]:
        c.start()
    for c in b1:
        c.wait_recv()
    for c in b2[:2] + w2[:2] + told + asks[:EARLY]:
        c.start()
    vals[128:144, :] = jnp.ones((16, 4096), bf16)

    def build(bz, by):
        b = bz * 4 + by
        start = pl.multiple_of(b * 256, 256)
        rows = pl.ds(start, 256)
        lat = jnp.concatenate([la[bz, by], lb[bz, by, 0:256, :]], axis=1)
        keys[rows, 0:128] = jnp.dot(lat, up_k[...], preferred_element_type=f32).astype(bf16)
        vals[0:128, rows] = lax.dot_general(
            up_vt[...], lat, (((1,), (1,)), ((), ())), preferred_element_type=f32
        ).astype(bf16)
        turn = lb[bz, by, 256:384, :].astype(f32)
        keys[pl.ds(start, 128), 128:256] = turn.astype(bf16)
        keys[pl.ds(pl.multiple_of(start + 128, 128), 128), 128:256] = pltpu.roll(turn, 64, 1).astype(bf16)

    for n in range(2):
        a2[n].wait_recv()
        a2[n + 2].start()
    for n in range(2):
        b2[n].wait_recv()
        b2[n + 2].start()
    for n in range(2):
        w2[n].wait_recv()
        w2[n + 2].start()
        for c in to_x(2 * n + 1) + [to_core(2 * n + 1, 0)]:
            c.start()
    for c in asks[EARLY:]:
        c.start()

    @pl.loop(0, 9)
    def _(n):
        build(lax.rem(z + 3 + n // 3, 4), lax.rem(y + 3 + lax.rem(n, 3), 4))

    for c in a2[2:] + b2[2:]:
        c.wait_recv()

    @pl.loop(0, 4)
    def _(n):
        build(zo, lax.rem(y + n, 4))

    @pl.loop(0, 3)
    def _(n):
        build(lax.rem(z + 3 + n, 4), yo)

    unit = 192.0 ** -0.5 * math.log2(math.e)
    mine = pl.ds(pl.multiple_of(me * 128, 128), 128)

    def one_pair(r, _):
        dz, dj = (PZ >> (2 * r)) & 3, (PJ >> (2 * r)) & 3
        pair = lax.rem(z + dz, 4) * 2 + lax.rem(y // 2 + dj, 2)
        for e in range(2):
            source = 2 * pair + e

            @pl.when(source != me)
            def _(source=source):
                remote(q_in.at[source], q_in.at[source], sq.at[0], rq.at[source], source).wait_recv()

        @pl.when(r == 2)
        def _():
            for c in w2[2:]:
                c.wait_recv()
            for c in to_x(2) + [to_core(2, 0)]:
                c.start()

        for i, g in enumerate((0, 1, 3)):

            @pl.when(r == 2 * i + 3)
            def _(g=g):
                for d in (1, 2, 3):
                    to_x(g)[d - 1].wait_recv()
                    to_core(g, d).start()

        q = jnp.concatenate([q_in[2 * pair], q_in[2 * pair + 1]], axis=1)

        def scores(at):
            return jnp.dot(keys[pl.ds(at, 512), 0:192], q, preferred_element_type=f32)

        def weigh(s, at, top, acc):
            new = jnp.maximum(top, jnp.max(s, axis=0, keepdims=True) * unit)
            p = jnp.exp2(s * unit - new).astype(bf16)
            return new, acc * jnp.exp2(top - new) + jnp.dot(
                vals[:, pl.ds(at, 512)], p, preferred_element_type=f32
            )

        last = pl.multiple_of(pair * 512, 512)
        key_id = lax.broadcasted_iota(i32, (512, 512), 0)
        row_id = lax.broadcasted_iota(i32, (512, 512), 1)
        s = jnp.where(key_id <= row_id, scores(last), masked_score)
        top = jnp.max(s, axis=0, keepdims=True) * unit
        p = jnp.exp2(s * unit - top).astype(bf16)
        acc = jnp.dot(vals[:, pl.ds(last, 512)], p, preferred_element_type=f32)

        def single(i, carry):
            at = pl.multiple_of((pair - 1) * 512, 512)
            return weigh(scores(at), at, *carry)

        def double(i, carry):
            at = pl.multiple_of(i * 1024, 1024)
            then = pl.multiple_of(at + 512, 512)
            s, t = scores(at), scores(then)
            return weigh(t, then, *weigh(s, at, *carry))

        carry = lax.fori_loop(0, lax.rem(pair, 2), single, (top, acc))
        top, acc = lax.fori_loop(0, pair // 2, double, carry)
        rows = acc[0:128] / acc[128:129]
        for e in range(2):
            attended[2 * r + e] = rows[:, 256 * e : 256 * e + 256].T.astype(bf16)
        for e in range(2):
            source = 2 * pair + e

            @pl.when(source != me)
            def _(e=e, source=source):
                remote(attended.at[2 * r + e], heads.at[:, mine], so.at[2 * r + e], ro.at[me], source).start()

            @pl.when(source == me)
            def _(e=e):
                heads[:, mine] = attended[2 * r + e]

        return 0

    lax.fori_loop(0, 8, one_pair, 0)
    for d in (1, 2, 3):
        to_x(2)[d - 1].wait_recv()
        to_core(2, d).start()
    for k in range(1, 16):
        head = along(*ORDER[k])
        there = pl.ds(pl.multiple_of(head * 128, 128), 128)
        remote(attended.at[0], heads.at[:, there], so.at[0], ro.at[head], head).wait_recv()
    for g in range(4):
        for d in range(4):
            to_core(g, d).wait_recv()

    @pl.loop(0, 8)
    def _(n):
        cols = pl.ds(pl.multiple_of(n * 256, 256), 256)
        p = jnp.dot(heads[...], wo[n].reshape(2048, 256), preferred_element_type=f32).astype(bf16)
        out[:, cols] = resid[:, cols].astype(f32) + p.astype(f32)

    @pl.loop(0, 8)
    def _(r):
        rows = pl.ds(pl.multiple_of(r * 32, 32), 32)
        a = out[rows, :]
        scale = lax.rsqrt(jnp.mean(a * a, axis=-1, keepdims=True) + epsilon)
        full = (a * scale * gain[...]).astype(bf16)
        shared[0, 0, rows, :] = full[:, 0:1024]
        shared[1, 0, rows, :] = full[:, 1024:2048]

    def line(h, d):
        return along(0, d) if h == 0 else along(d, 0)

    def cross(h, d):
        return along(d, 0) if h == 0 else along(0, d)

    def slots_of(h):
        r = lax.broadcasted_iota(i32, (256, 1), 0)
        owner = [cross(h, d) * 64 for d in range(4)]
        base = jnp.where(r < 64, owner[0], jnp.where(r < 128, owner[1], jnp.where(r < 192, owner[2], owner[3])))
        return (base + (r & 63)).astype(f32)

    share = []
    for h in range(2):
        at = lambda n, h=h: (ssh.at[4 * h + n], rsh.at[4 * h + n])
        share.append(
            [
                remote(shared.at[h, 0], shared.at[h, 1], *at(0), line(h, 1)),
                remote(shared.at[h, 0], shared.at[h, 2], *at(1), line(h, 3)),
                remote(shared.at[h, 1, 0:128], shared.at[h, 3, 0:128], *at(2), line(h, 1)),
                remote(shared.at[h, 2, 128:256], shared.at[h, 3, 128:256], *at(3), line(h, 3)),
            ]
        )
    for n in range(2):
        for h in range(2):
            share[h][n].start()
    for c in told:
        c.wait_recv()
    for load in loads:
        load.wait()

    def dealt(h, d, a):
        there = arrived.at[0, PLACE[d], a] if h == 0 else arrived.at[1, a, PLACE[d]]
        n = 16 * h + 4 * d + a
        return remote(outgoing.at[h, d, a], there, sd.at[n], rd.at[n], cross(h, d))

    def deal(a):
        for h in range(2):
            place = slots_of(h)
            pick = (place == told_all[h, a, 0:1, :]) | (place == told_all[h, a, 1:2, :])
            pick = jnp.where(pick, 1.0, 0.0).astype(bf16)
            for n in range(2):
                cols = slice(n * 512, n * 512 + 512)
                rows = jnp.dot(pick, shared[h, a, :, cols], preferred_element_type=f32).astype(bf16)
                if h == 0:
                    arrived[0, 0, a, :, cols] = rows[0:64]
                else:
                    arrived[1, a, 0, :, cols] = rows[0:64]
                for d in (1, 2, 3):
                    outgoing[h, d, a, :, cols] = rows[64 * d : 64 * d + 64]
        for d in (2, 1, 3):
            for h in range(2):
                dealt(h, d, a).start()

    deal(0)
    for n in range(2):
        for h in range(2):
            share[h][n].wait_recv()
            share[h][n + 2].start()
    deal(1)
    deal(2)
    for n in (2, 3):
        for h in range(2):
            share[h][n].wait_recv()
    deal(3)

    def given(h, d, a):
        zp, yp = (PLACE[d], a) if h == 0 else (a, PLACE[d])
        n = 16 * h + 4 * d + a
        return remote(result.at[h, zp, yp], returned.at[h, d, a], sg.at[n], rg.at[n], cross(h, 4 - d))

    for i, j in ((0, 0), (0, 1), (1, 0), (1, 1)):
        zs, ys = (2 * i, 2 * i + 1), (2 * j, 2 * j + 1)
        for zp in zs:
            for yp in ys:
                if zp > 0:
                    dealt(0, SHIFT[zp], yp).wait_recv()
                if yp > 0:
                    dealt(1, SHIFT[yp], zp).wait_recv()

        @pl.loop(0, 4)
        def _(n):
            cols = pl.ds(pl.multiple_of(n * 256, 256), 256)
            r0 = arrived[0, 2 * i : 2 * i + 2, 2 * j : 2 * j + 2].reshape(256, 1024)
            r1 = arrived[1, 2 * i : 2 * i + 2, 2 * j : 2 * j + 2].reshape(256, 1024)
            gate = jnp.dot(r0, wg[0:1024, cols], preferred_element_type=f32)
            gate = gate + jnp.dot(r1, wg[1024:2048, cols], preferred_element_type=f32)
            up = jnp.dot(r0, wu[0:1024, cols], preferred_element_type=f32)
            up = up + jnp.dot(r1, wu[1024:2048, cols], preferred_element_type=f32)
            hidden[:, cols] = (gate / (1.0 + jnp.exp(-gate)) * up).astype(bf16)

        for h in range(2):

            @pl.loop(0, 2)
            def _(n, h=h):
                cols = pl.ds(pl.multiple_of(n * 512, 512), 512)
                wide = pl.ds(pl.multiple_of(n * 512 + h * 1024, 512), 512)
                rows = jnp.dot(hidden[...], wd[:, wide], preferred_element_type=f32).astype(bf16)
                for p, zp in enumerate(zs):
                    for q, yp in enumerate(ys):
                        part = rows[128 * p + 64 * q : 128 * p + 64 * q + 64]
                        if h == 0 and zp == 0:
                            returned[0, 0, yp, :, cols] = part
                        elif h == 1 and yp == 0:
                            returned[1, 0, zp, :, cols] = part
                        else:
                            result[h, zp, yp, :, cols] = part

            for zp in zs:
                for yp in ys:
                    if h == 0 and zp > 0:
                        given(0, SHIFT[zp], yp).start()
                    if h == 1 and yp > 0:
                        given(1, SHIFT[yp], zp).start()

    for h in range(2):
        for c in share[h]:
            c.wait_send()

    def summed(h, a):
        n = 3 * h + a - 1
        return remote(shared.at[h, a], final.at[h, a - 1], sf.at[n], rf.at[n], line(h, 4 - SHIFT[a]))

    for a in (1, 2, 3, 0):
        for h in range(2):
            for d in (1, 2, 3):
                given(h, d, a).wait_recv()
            place = slots_of(h)
            share_of = jnp.where(place == told_all[h, a, 0:1, :], told_all[h, a, 2:3, :], 0.0)
            share_of = share_of + jnp.where(place == told_all[h, a, 1:2, :], told_all[h, a, 3:4, :], 0.0)
            share_of = share_of.T
            high = share_of.astype(bf16)
            low = (share_of - high.astype(f32)).astype(bf16)
            for n in range(2):
                cols = slice(n * 512, n * 512 + 512)
                rows = returned[h, :, a, :, cols].reshape(256, 512)
                t = jnp.dot(high, rows, preferred_element_type=f32) + jnp.dot(low, rows, preferred_element_type=f32)
                if a == 0:
                    wide = slice(h * 1024 + n * 512, h * 1024 + n * 512 + 512)
                    out[:, wide] = out[:, wide] + t
                else:
                    shared[h, a, :, cols] = t.astype(bf16)
            if a > 0:
                summed(h, a).start()
    for h in range(2):
        for a in (1, 2, 3):
            summed(h, a).wait_recv()
        wide = slice(h * 1024, h * 1024 + 1024)
        t = out[:, wide]
        for n in range(3):
            t = t + final[h, n].astype(f32)
        out[:, wide] = t
    for h in range(2):
        for a in range(4):
            for d in (1, 2, 3):
                dealt(h, d, a).wait_send()
                given(h, d, a).wait_send()
        for a in (1, 2, 3):
            summed(h, a).wait_send()
    for c in told + a1 + b1 + w1 + a2 + b2 + w2 + asks:
        c.wait_send()
    for n in range(16):

        @pl.when(lax.rem(y, 2) != n)
        def _(n=n):
            remote(attended.at[n], heads.at[:, mine], so.at[n], ro.at[me], me).wait_send()

    for g in range(4):
        for c in to_x(g) + [to_core(g, d) for d in range(4)]:
            c.wait_send()


def layer(nope, rope_t, lat, lat_gain, key_t, cos, sin, up_k, up_v, wo, resid, gain, routes_t, weight_t, wg, wu, wd):
    v, a = pl.BlockSpec(memory_space=pltpu.VMEM), pl.BlockSpec(memory_space=pl.ANY)
    bf16, f32 = jnp.bfloat16, jnp.float32
    dma = pltpu.SemaphoreType.DMA
    return pl.pallas_call(
        layer_kernel,
        name="layer",
        out_shape=jax.ShapeDtypeStruct((256, 2048), f32),
        in_specs=[v] * 9 + [a] + [v] * 4 + [a] * 3,
        out_specs=v,
        scratch_shapes=[
            pltpu.VMEM((2048, 1024), bf16),
            pltpu.VMEM((2048, 1024), bf16),
            pltpu.VMEM((1024, 2048), bf16),
            pltpu.VMEM((2, 4, 8, 256), f32),
            pltpu.VMEM((2, 4, 256, 1024), bf16),
            pltpu.VMEM((2, 4, 4, 64, 1024), bf16),
            pltpu.VMEM((2, 4, 4, 64, 1024), bf16),
            pltpu.VMEM((256, 1024), bf16),
            pltpu.VMEM((2, 4, 4, 64, 1024), bf16),
            pltpu.VMEM((2, 4, 4, 64, 1024), bf16),
            pltpu.VMEM((2, 3, 256, 1024), bf16),
            pltpu.VMEM((16, 192, 256), bf16),
            pltpu.VMEM((16, 192, 256), bf16),
            pltpu.VMEM((4, 4, 256, 128), bf16),
            pltpu.VMEM((4, 4, 384, 128), bf16),
            pltpu.VMEM((128, 256), bf16),
            pltpu.VMEM((4096, 256), bf16),
            pltpu.VMEM((144, 4096), bf16),
            pltpu.VMEM((16, 256, 128), bf16),
            pltpu.VMEM((256, 2048), bf16),
            pltpu.VMEM((8, 4, 4, 128, 256), bf16),
            dma((3,)),
        ]
        + [dma((8,))] * 4
        + [dma((32,))] * 4
        + [dma((6,))] * 2
        + [dma((4,))] * 9
        + [dma((16,))] * 4
        + [dma((4,))] * 4
        + [dma((4, 4))] * 4,
        compiler_params=pltpu.CompilerParams(
            collective_id=1, has_side_effects=True, vmem_limit_bytes=65400 * 1024
        ),
    )(nope, rope_t, lat, lat_gain, key_t, cos, sin, up_k, up_v, wo, resid, gain, routes_t, weight_t, wg, wu, wd)


def shards(
    query_nope,
    query_rope,
    latent,
    key_rope,
    resid,
    latent_gain,
    key_up,
    value_up,
    out_proj,
    norm_gain,
    expert_gate,
    expert_up,
    expert_down,
    routes,
    route_weight,
):
    tokens = latent.shape[1]
    positions = lax.axis_index("sp") * tokens + jnp.arange(tokens, dtype=jnp.int32)
    half_width = key_rope.shape[-1] // 2
    frequency = rope_base ** (-jnp.arange(half_width, dtype=jnp.float32) / half_width)
    angles = frequency[:, None] * positions.astype(jnp.float32)[None, :]
    return layer(
        query_nope[0], query_rope[0].transpose(1, 2, 0), latent[0], latent_gain[None],
        key_rope[0].T, jnp.cos(angles), jnp.sin(angles), key_up, value_up, out_proj, resid[0], norm_gain[None],
        routes[0].T, route_weight[0].T, expert_gate[0], expert_up[0], expert_down[0],
    ).astype(jnp.bfloat16)[None]


def solution(mesh):
    return jax.shard_map(
        shards,
        mesh=mesh,
        in_specs=(
            P("dp", "sp", None, None),
            P("dp", "sp", None, None),
            P("dp", "sp", None),
            P("dp", "sp", None),
            P("dp", "sp", None),
            P(),
            P(None, "sp"),
            P(None, "sp"),
            P("sp", "dp"),
            P(),
            P("sp", None, None),
            P("sp", None, None),
            P("sp", None, None),
            P("dp", "sp", None),
            P("dp", "sp", None),
        ),
        out_specs=P("dp", "sp", None),
        check_vma=False,
    )
```

```python
import math

import jax
import jax.numpy as jnp
from jax import lax
from jax.experimental import pallas as pl
from jax.experimental.pallas import tpu as pltpu
from jax.sharding import PartitionSpec as P

epsilon = 1e-06
rope_base = 10000.0
masked_score = -1e30


ORDER = [(0, 0), (2, 2), (3, 2), (2, 3), (1, 2), (2, 1), (0, 2), (2, 0), (3, 1), (1, 3), (3, 3), (1, 1), (3, 0), (0, 3), (1, 0), (0, 1)]
MESH = pl.DeviceIdType.MESH


def packed(digits):
    value = sum(d << (2 * i) for i, d in enumerate(digits))
    return value - (1 << 32) if value >= 1 << 31 else value


PLACE = {0: 0, 1: 1, 3: 2, 2: 3}
EARLY = 3
SHIFT = [0, 1, 3, 2]
PAIRS = [(0, 0), (2, 1), (1, 1), (3, 1), (2, 0), (0, 1), (1, 0), (3, 0)]
PZ, PJ = packed([o[0] for o in PAIRS]), packed([o[1] for o in PAIRS])


def shifted(me, dz, dy):
    z, y = me // 4, lax.rem(me, 4)
    return lax.rem(z + dz, 4) * 4 + lax.rem(y + dy, 4)


def remote(src, dst, send, recv, target):
    return pltpu.make_async_remote_copy(
        src_ref=src,
        dst_ref=dst,
        send_sem=send,
        recv_sem=recv,
        device_id={"sp": target},
        device_id_type=MESH,
    )


def layer_kernel(
    nope, rope_t, lat_in, lat_gain, key_t, cosine, sine, up_k, up_v, wo_hbm, resid, gain, routes_t, weight_t, wg_hbm, wu_hbm, wd_hbm, out,
    wg, wu, wd, told_all, shared, outgoing, arrived, hidden, result, returned, final, halfway,
    q_out, q_in, la, lb, up_vt, keys, vals, attended, heads, wo,
    wsem, st, rt, ssh, rsh, sd, rd, sg, rg, sf, rf,
    lsem, sa1, ra1, sb1, rb1, sa2, ra2, sb2, rb2, sq, rq, so, ro, swz, rwz, swy, rwy, swx, rwx, swc, rwc,
):
    me, dp = lax.axis_index("sp"), lax.axis_index("dp")
    z, y = me // 4, lax.rem(me, 4)
    x, core = dp // 2, lax.rem(dp, 2)
    f32, bf16, i32 = jnp.float32, jnp.bfloat16, jnp.int32
    barrier = pltpu.get_barrier_semaphore()
    for dz, dy in ORDER[1:]:
        pl.semaphore_signal(barrier, inc=1, device_id={"sp": shifted(me, dz, dy)}, device_id_type=MESH)
    x_peer = [None] + [lax.rem(x + d, 4) * 2 + core for d in (1, 2, 3)]
    x_from = [dp] + [lax.rem(x + 4 - d, 4) * 2 + core for d in (1, 2, 3)]
    other = x * 2 + 1 - core
    for t in x_peer[1:] + [other]:
        pl.semaphore_signal(barrier, inc=1, device_id={"dp": t}, device_id_type=MESH)
    fill_wo = pltpu.make_async_copy(wo_hbm, wo.at[dp, z, y], lsem.at[0])
    fill_wo.start()
    loads = [
        pltpu.make_async_copy(a, b, wsem.at[i])
        for i, (a, b) in enumerate(((wg_hbm, wg), (wu_hbm, wu), (wd_hbm, wd)))
    ]
    for load in loads:
        load.start()
    tok = lax.broadcasted_iota(i32, (256, 256), 0)
    tok_l = lax.broadcasted_iota(i32, (256, 256), 1)
    upper = jnp.where(tok < tok_l, 1.0, 0.0).astype(bf16)
    expert = lax.broadcasted_iota(i32, (16, 256), 0).astype(f32)
    hot = [jnp.where(expert == routes_t[k : k + 1, :].astype(f32), 1.0, 0.0) for k in range(2)]
    before = jnp.dot((hot[0] + hot[1]).astype(bf16), upper, preferred_element_type=f32) + expert * 64.0
    for h in range(2):
        for k in range(2):
            told_all[h, 0, k : k + 1, :] = jnp.sum(hot[k] * before, axis=0, keepdims=True)
        told_all[h, 0, 2:4, :] = weight_t[...]
        told_all[h, 0, 4:8, :] = jnp.zeros((4, 256), f32)

    lat = lat_in[...].astype(f32)
    lat = lat * lax.rsqrt(jnp.mean(lat * lat, axis=-1, keepdims=True) + epsilon) * lat_gain[...]
    la[z, y] = lat[:, 0:128].astype(bf16)
    lb[z, y, 0:256, :] = lat[:, 128:256].astype(bf16)
    cos, sin = cosine[...], sine[...]
    a, b = key_t[0:32, :].astype(f32), key_t[32:64, :].astype(f32)
    turned = jnp.concatenate([a * cos - b * sin, b * cos + a * sin], axis=0)
    lb[z, y, 256:384, :] = jnp.concatenate([turned[:, 0:128], turned[:, 128:256]], axis=0).T.astype(bf16)
    up_vt[...] = up_v[...].astype(f32).T.astype(bf16)

    fill_wo.wait()
    pl.semaphore_wait(barrier, 19)

    def along(dz, dy):
        return shifted(me, dz, dy)

    told = []
    for h in range(2):
        for d in (1, 2, 3):
            target = along(0, d) if h == 0 else along(d, 0)
            told.append(remote(told_all.at[h, 0], told_all.at[h, PLACE[d]], st.at[4 * h + d], rt.at[4 * h + d], target))
    a1 = [remote(la.at[z, y], la.at[z, y], sa1.at[d], ra1.at[d], along(d, 0)) for d in (1, 2, 3)]
    b1 = [remote(lb.at[z, y], lb.at[z, y], sb1.at[d], rb1.at[d], along(0, d)) for d in (1, 2, 3)]
    w1 = [remote(wo.at[dp, z, y], wo.at[dp, z, y], swz.at[d], rwz.at[d], along(d, 0)) for d in (1, 2, 3)]
    ym, yp, yo = [lax.rem(y + n, 4) for n in (3, 1, 2)]
    zm, zp, zo = [lax.rem(z + n, 4) for n in (3, 1, 2)]
    up, down, fore, back = along(0, 1), along(0, 3), along(1, 0), along(3, 0)
    a2 = [
        remote(la.at[:, y], la.at[:, y], sa2.at[0], ra2.at[0], up),
        remote(la.at[:, y], la.at[:, y], sa2.at[1], ra2.at[1], down),
        remote(la.at[0:2, ym], la.at[0:2, ym], sa2.at[2], ra2.at[2], up),
        remote(la.at[2:4, yp], la.at[2:4, yp], sa2.at[3], ra2.at[3], down),
    ]
    b2 = [
        remote(lb.at[z], lb.at[z], sb2.at[0], rb2.at[0], fore),
        remote(lb.at[z], lb.at[z], sb2.at[1], rb2.at[1], back),
        remote(lb.at[zm, 0:2], lb.at[zm, 0:2], sb2.at[2], rb2.at[2], fore),
        remote(lb.at[zp, 2:4], lb.at[zp, 2:4], sb2.at[3], rb2.at[3], back),
    ]
    w2 = [
        remote(wo.at[dp, :, y], wo.at[dp, :, y], swy.at[0], rwy.at[0], up),
        remote(wo.at[dp, :, y], wo.at[dp, :, y], swy.at[1], rwy.at[1], down),
        remote(wo.at[dp, 0:2, ym], wo.at[dp, 0:2, ym], swy.at[2], rwy.at[2], up),
        remote(wo.at[dp, 2:4, yp], wo.at[dp, 2:4, yp], swy.at[3], rwy.at[3], down),
    ]
    asks = []
    for r, (dz, dj) in enumerate(PAIRS):
        for e in range(2):
            if r == 0:
                target = me + 1 - 2 * lax.rem(y, 2)
                if e == 1:
                    continue
            else:
                target = lax.rem(z + 4 - dz, 4) * 4 + lax.rem(y // 2 + dj, 2) * 2 + e
            asks.append(remote(q_out.at[target], q_in.at[me], sq.at[2 * r + e], rq.at[me], target))

    def to_x(g):
        part = wo.at[dp, :, lax.rem(y + 4 - g, 4)]
        copies = [
            pltpu.make_async_remote_copy(
                src_ref=part, dst_ref=part, send_sem=swx.at[g, d], recv_sem=rwx.at[g, d],
                device_id={"dp": x_peer[d]}, device_id_type=MESH,
            )
            for d in (1, 2, 3)
        ]
        return copies

    def to_core(g, d):
        part = wo.at[x_from[d], :, lax.rem(y + 4 - g, 4)]
        return pltpu.make_async_remote_copy(
            src_ref=part, dst_ref=part, send_sem=swc.at[g, d], recv_sem=rwc.at[g, d],
            device_id={"dp": other}, device_id_type=MESH,
        )

    for c in w1 + a1 + b1:
        c.start()
    for t in (0, 128):
        by_head = nope[t : t + 128].astype(f32).transpose(1, 0, 2)
        for h in range(16):
            q_out[h, 0:128, t : t + 128] = by_head[h].T.astype(bf16)

    @pl.loop(0, 16)
    def _(h):
        a, b = rope_t[h, 0:32, :].astype(f32), rope_t[h, 32:64, :].astype(f32)
        q_out[h, 128:160, :] = (a * cosine[...] - b * sine[...]).astype(bf16)
        q_out[h, 160:192, :] = (b * cosine[...] + a * sine[...]).astype(bf16)

    q_in[me] = q_out[me]
    for c in w1:
        c.wait_recv()
    for c in to_x(0) + [to_core(0, 0)]:
        c.start()
    for c in a1:
        c.wait_recv()
    for c in a2[:2]:
        c.start()
    for c in b1:
        c.wait_recv()
    for c in b2[:2] + w2[:2] + told + asks[:EARLY]:
        c.start()
    vals[128:144, :] = jnp.ones((16, 4096), bf16)

    def build(bz, by):
        b = bz * 4 + by
        start = pl.multiple_of(b * 256, 256)
        rows = pl.ds(start, 256)
        lat = jnp.concatenate([la[bz, by], lb[bz, by, 0:256, :]], axis=1)
        keys[rows, 0:128] = jnp.dot(lat, up_k[...], preferred_element_type=f32).astype(bf16)
        vals[0:128, rows] = lax.dot_general(
            up_vt[...], lat, (((1,), (1,)), ((), ())), preferred_element_type=f32
        ).astype(bf16)
        turn = lb[bz, by, 256:384, :].astype(f32)
        keys[pl.ds(start, 128), 128:256] = turn.astype(bf16)
        keys[pl.ds(pl.multiple_of(start + 128, 128), 128), 128:256] = pltpu.roll(turn, 64, 1).astype(bf16)

    for n in range(2):
        a2[n].wait_recv()
        a2[n + 2].start()
    for n in range(2):
        b2[n].wait_recv()
        b2[n + 2].start()
    for n in range(2):
        w2[n].wait_recv()
        w2[n + 2].start()
        for c in to_x(2 * n + 1) + [to_core(2 * n + 1, 0)]:
            c.start()
    for c in asks[EARLY:]:
        c.start()

    @pl.loop(0, 9)
    def _(n):
        build(lax.rem(z + 3 + n // 3, 4), lax.rem(y + 3 + lax.rem(n, 3), 4))

    for c in a2[2:] + b2[2:]:
        c.wait_recv()

    @pl.loop(0, 4)
    def _(n):
        build(zo, lax.rem(y + n, 4))

    @pl.loop(0, 3)
    def _(n):
        build(lax.rem(z + 3 + n, 4), yo)

    unit = 192.0 ** -0.5 * math.log2(math.e)
    mine = pl.ds(pl.multiple_of(me * 128, 128), 128)

    def one_pair(r, _):
        dz, dj = (PZ >> (2 * r)) & 3, (PJ >> (2 * r)) & 3
        pair = lax.rem(z + dz, 4) * 2 + lax.rem(y // 2 + dj, 2)
        for e in range(2):
            source = 2 * pair + e

            @pl.when(source != me)
            def _(source=source):
                remote(q_in.at[source], q_in.at[source], sq.at[0], rq.at[source], source).wait_recv()

        @pl.when(r == 2)
        def _():
            for c in w2[2:]:
                c.wait_recv()
            for c in to_x(2) + [to_core(2, 0)]:
                c.start()

        for i, g in enumerate((0, 1, 3)):

            @pl.when(r == 2 * i + 3)
            def _(g=g):
                for d in (1, 2, 3):
                    to_x(g)[d - 1].wait_recv()
                    to_core(g, d).start()

        q = jnp.concatenate([q_in[2 * pair], q_in[2 * pair + 1]], axis=1)

        def scores(at):
            return jnp.dot(keys[pl.ds(at, 512), 0:192], q, preferred_element_type=f32)

        def weigh(s, at, top, acc):
            new = jnp.maximum(top, jnp.max(s, axis=0, keepdims=True) * unit)
            p = jnp.exp2(s * unit - new).astype(bf16)
            return new, acc * jnp.exp2(top - new) + jnp.dot(
                vals[:, pl.ds(at, 512)], p, preferred_element_type=f32
            )

        last = pl.multiple_of(pair * 512, 512)
        key_id = lax.broadcasted_iota(i32, (512, 512), 0)
        row_id = lax.broadcasted_iota(i32, (512, 512), 1)
        s = jnp.where(key_id <= row_id, scores(last), masked_score)
        top = jnp.max(s, axis=0, keepdims=True) * unit
        p = jnp.exp2(s * unit - top).astype(bf16)
        acc = jnp.dot(vals[:, pl.ds(last, 512)], p, preferred_element_type=f32)

        def single(i, carry):
            at = pl.multiple_of((pair - 1) * 512, 512)
            return weigh(scores(at), at, *carry)

        def double(i, carry):
            at = pl.multiple_of(i * 1024, 1024)
            then = pl.multiple_of(at + 512, 512)
            s, t = scores(at), scores(then)
            return weigh(t, then, *weigh(s, at, *carry))

        carry = lax.fori_loop(0, lax.rem(pair, 2), single, (top, acc))
        top, acc = lax.fori_loop(0, pair // 2, double, carry)
        rows = acc[0:128] / acc[128:129]
        for e in range(2):
            attended[2 * r + e] = rows[:, 256 * e : 256 * e + 256].T.astype(bf16)
        for e in range(2):
            source = 2 * pair + e

            @pl.when(source != me)
            def _(e=e, source=source):
                remote(attended.at[2 * r + e], heads.at[:, mine], so.at[2 * r + e], ro.at[me], source).start()

            @pl.when(source == me)
            def _(e=e):
                heads[:, mine] = attended[2 * r + e]

        return 0

    lax.fori_loop(0, 8, one_pair, 0)
    for d in (1, 2, 3):
        to_x(2)[d - 1].wait_recv()
        to_core(2, d).start()
    for k in range(1, 16):
        head = along(*ORDER[k])
        there = pl.ds(pl.multiple_of(head * 128, 128), 128)
        remote(attended.at[0], heads.at[:, there], so.at[0], ro.at[head], head).wait_recv()
    for g in range(4):
        for d in range(4):
            to_core(g, d).wait_recv()

    @pl.loop(0, 8)
    def _(n):
        cols = pl.ds(pl.multiple_of(n * 256, 256), 256)
        p = jnp.dot(heads[...], wo[n].reshape(2048, 256), preferred_element_type=f32).astype(bf16)
        out[:, cols] = resid[:, cols].astype(f32) + p.astype(f32)

    @pl.loop(0, 8)
    def _(r):
        rows = pl.ds(pl.multiple_of(r * 32, 32), 32)
        a = out[rows, :]
        scale = lax.rsqrt(jnp.mean(a * a, axis=-1, keepdims=True) + epsilon)
        full = (a * scale * gain[...]).astype(bf16)
        shared[0, 0, rows, :] = full[:, 0:1024]
        shared[1, 0, rows, :] = full[:, 1024:2048]

    def line(h, d):
        return along(0, d) if h == 0 else along(d, 0)

    def cross(h, d):
        return along(d, 0) if h == 0 else along(0, d)

    def slots_of(h):
        r = lax.broadcasted_iota(i32, (256, 1), 0)
        owner = [cross(h, d) * 64 for d in range(4)]
        base = jnp.where(r < 64, owner[0], jnp.where(r < 128, owner[1], jnp.where(r < 192, owner[2], owner[3])))
        return (base + (r & 63)).astype(f32)

    share = []
    for h in range(2):
        at = lambda n, h=h: (ssh.at[4 * h + n], rsh.at[4 * h + n])
        share.append(
            [
                remote(shared.at[h, 0], shared.at[h, 1], *at(0), line(h, 1)),
                remote(shared.at[h, 0], shared.at[h, 2], *at(1), line(h, 3)),
                remote(shared.at[h, 1, 0:128], shared.at[h, 3, 0:128], *at(2), line(h, 1)),
                remote(shared.at[h, 2, 128:256], shared.at[h, 3, 128:256], *at(3), line(h, 3)),
            ]
        )
    for n in range(2):
        for h in range(2):
            share[h][n].start()
    for c in told:
        c.wait_recv()
    for load in loads:
        load.wait()

    def dealt(h, d, a):
        there = arrived.at[0, PLACE[d], a] if h == 0 else arrived.at[1, a, PLACE[d]]
        n = 16 * h + 4 * d + a
        return remote(outgoing.at[h, d, a], there, sd.at[n], rd.at[n], cross(h, d))

    def deal(a):
        for h in range(2):
            place = slots_of(h)
            pick = (place == told_all[h, a, 0:1, :]) | (place == told_all[h, a, 1:2, :])
            pick = jnp.where(pick, 1.0, 0.0).astype(bf16)
            for n in range(2):
                cols = slice(n * 512, n * 512 + 512)
                rows = jnp.dot(pick, shared[h, a, :, cols], preferred_element_type=f32).astype(bf16)
                if h == 0:
                    arrived[0, 0, a, :, cols] = rows[0:64]
                else:
                    arrived[1, a, 0, :, cols] = rows[0:64]
                for d in (1, 2, 3):
                    outgoing[h, d, a, :, cols] = rows[64 * d : 64 * d + 64]
        for d in (2, 1, 3):
            for h in range(2):
                dealt(h, d, a).start()

    deal(0)
    for n in range(2):
        for h in range(2):
            share[h][n].wait_recv()
            share[h][n + 2].start()
    deal(1)
    deal(2)
    for n in (2, 3):
        for h in range(2):
            share[h][n].wait_recv()
    deal(3)

    def given(h, d, a):
        zp, yp = (PLACE[d], a) if h == 0 else (a, PLACE[d])
        n = 16 * h + 4 * d + a
        return remote(result.at[h, zp, yp], returned.at[h, d, a], sg.at[n], rg.at[n], cross(h, 4 - d))

    for i, j in ((0, 0), (0, 1), (1, 0), (1, 1)):
        zs, ys = (2 * i, 2 * i + 1), (2 * j, 2 * j + 1)
        for zp in zs:
            for yp in ys:
                if zp > 0:
                    dealt(0, SHIFT[zp], yp).wait_recv()
                if yp > 0:
                    dealt(1, SHIFT[yp], zp).wait_recv()

        @pl.loop(0, 4)
        def _(n):
            cols = pl.ds(pl.multiple_of(n * 256, 256), 256)
            r0 = arrived[0, 2 * i : 2 * i + 2, 2 * j : 2 * j + 2].reshape(256, 1024)
            r1 = arrived[1, 2 * i : 2 * i + 2, 2 * j : 2 * j + 2].reshape(256, 1024)
            gate = jnp.dot(r0, wg[0:1024, cols], preferred_element_type=f32)
            gate = gate + jnp.dot(r1, wg[1024:2048, cols], preferred_element_type=f32)
            up = jnp.dot(r0, wu[0:1024, cols], preferred_element_type=f32)
            up = up + jnp.dot(r1, wu[1024:2048, cols], preferred_element_type=f32)
            hidden[:, cols] = (gate / (1.0 + jnp.exp(-gate)) * up).astype(bf16)

        for h in range(2):

            @pl.loop(0, 2)
            def _(n, h=h):
                cols = pl.ds(pl.multiple_of(n * 512, 512), 512)
                wide = pl.ds(pl.multiple_of(n * 512 + h * 1024, 512), 512)
                rows = jnp.dot(hidden[...], wd[:, wide], preferred_element_type=f32).astype(bf16)
                for p, zp in enumerate(zs):
                    for q, yp in enumerate(ys):
                        part = rows[128 * p + 64 * q : 128 * p + 64 * q + 64]
                        if h == 0 and zp == 0:
                            returned[0, 0, yp, :, cols] = part
                        elif h == 1 and yp == 0:
                            returned[1, 0, zp, :, cols] = part
                        else:
                            result[h, zp, yp, :, cols] = part

            for zp in zs:
                for yp in ys:
                    if h == 0 and zp > 0:
                        given(0, SHIFT[zp], yp).start()
                    if h == 1 and yp > 0:
                        given(1, SHIFT[yp], zp).start()

    for h in range(2):
        for c in share[h]:
            c.wait_send()

    def summed(h, a):
        n = 4 * h + a - 1
        return remote(shared.at[h, a], final.at[h, a - 1], sf.at[n], rf.at[n], line(h, 4 - SHIFT[a]))

    def crossing(h, n):
        at = 4 * h + 2 + n
        half = shared.at[h, 3, 128 * n : 128 * n + 128]
        return remote(half, halfway.at[h, n], sf.at[at], rf.at[at], line(h, 1 + 2 * n))

    for a in (3, 1, 2, 0):
        for h in range(2):
            for d in (1, 2, 3):
                given(h, d, a).wait_recv()
            place = slots_of(h)
            share_of = jnp.where(place == told_all[h, a, 0:1, :], told_all[h, a, 2:3, :], 0.0)
            share_of = share_of + jnp.where(place == told_all[h, a, 1:2, :], told_all[h, a, 3:4, :], 0.0)
            share_of = share_of.T
            high = share_of.astype(bf16)
            low = (share_of - high.astype(f32)).astype(bf16)
            for n in range(2):
                cols = slice(n * 512, n * 512 + 512)
                rows = returned[h, :, a, :, cols].reshape(256, 512)
                t = jnp.dot(high, rows, preferred_element_type=f32) + jnp.dot(low, rows, preferred_element_type=f32)
                if a == 0:
                    wide = slice(h * 1024 + n * 512, h * 1024 + n * 512 + 512)
                    out[:, wide] = out[:, wide] + t
                else:
                    shared[h, a, :, cols] = t.astype(bf16)
            if a == 3:
                crossing(h, 0).start()
                crossing(h, 1).start()
    for h in range(2):
        for a in (1, 2):
            crossing(h, 2 - a).wait_recv()
            rows = slice(128, 256) if a == 1 else slice(0, 128)
            t = shared[h, a, rows, :].astype(f32) + halfway[h, 2 - a].astype(f32)
            shared[h, a, rows, :] = t.astype(bf16)
    for h in range(2):
        for a in (1, 2):
            summed(h, a).start()
    for h in range(2):
        for a in (1, 2):
            summed(h, a).wait_recv()
        wide = slice(h * 1024, h * 1024 + 1024)
        t = out[:, wide]
        for n in range(2):
            t = t + final[h, n].astype(f32)
        out[:, wide] = t
    for h in range(2):
        for a in range(4):
            for d in (1, 2, 3):
                dealt(h, d, a).wait_send()
                given(h, d, a).wait_send()
        for n in range(2):
            summed(h, n + 1).wait_send()
            crossing(h, n).wait_send()
    for c in told + a1 + b1 + w1 + a2 + b2 + w2 + asks:
        c.wait_send()
    for n in range(16):

        @pl.when(lax.rem(y, 2) != n)
        def _(n=n):
            remote(attended.at[n], heads.at[:, mine], so.at[n], ro.at[me], me).wait_send()

    for g in range(4):
        for c in to_x(g) + [to_core(g, d) for d in range(4)]:
            c.wait_send()


def layer(nope, rope_t, lat, lat_gain, key_t, cos, sin, up_k, up_v, wo, resid, gain, routes_t, weight_t, wg, wu, wd):
    v, a = pl.BlockSpec(memory_space=pltpu.VMEM), pl.BlockSpec(memory_space=pl.ANY)
    bf16, f32 = jnp.bfloat16, jnp.float32
    dma = pltpu.SemaphoreType.DMA
    return pl.pallas_call(
        layer_kernel,
        name="layer",
        out_shape=jax.ShapeDtypeStruct((256, 2048), f32),
        in_specs=[v] * 9 + [a] + [v] * 4 + [a] * 3,
        out_specs=v,
        scratch_shapes=[
            pltpu.VMEM((2048, 1024), bf16),
            pltpu.VMEM((2048, 1024), bf16),
            pltpu.VMEM((1024, 2048), bf16),
            pltpu.VMEM((2, 4, 8, 256), f32),
            pltpu.VMEM((2, 4, 256, 1024), bf16),
            pltpu.VMEM((2, 4, 4, 64, 1024), bf16),
            pltpu.VMEM((2, 4, 4, 64, 1024), bf16),
            pltpu.VMEM((256, 1024), bf16),
            pltpu.VMEM((2, 4, 4, 64, 1024), bf16),
            pltpu.VMEM((2, 4, 4, 64, 1024), bf16),
            pltpu.VMEM((2, 2, 256, 1024), bf16),
            pltpu.VMEM((2, 2, 128, 1024), bf16),
            pltpu.VMEM((16, 192, 256), bf16),
            pltpu.VMEM((16, 192, 256), bf16),
            pltpu.VMEM((4, 4, 256, 128), bf16),
            pltpu.VMEM((4, 4, 384, 128), bf16),
            pltpu.VMEM((128, 256), bf16),
            pltpu.VMEM((4096, 256), bf16),
            pltpu.VMEM((144, 4096), bf16),
            pltpu.VMEM((16, 256, 128), bf16),
            pltpu.VMEM((256, 2048), bf16),
            pltpu.VMEM((8, 4, 4, 128, 256), bf16),
            dma((3,)),
        ]
        + [dma((8,))] * 4
        + [dma((32,))] * 4
        + [dma((8,))] * 2
        + [dma((4,))] * 9
        + [dma((16,))] * 4
        + [dma((4,))] * 4
        + [dma((4, 4))] * 4,
        compiler_params=pltpu.CompilerParams(
            collective_id=1, has_side_effects=True, vmem_limit_bytes=65400 * 1024
        ),
    )(nope, rope_t, lat, lat_gain, key_t, cos, sin, up_k, up_v, wo, resid, gain, routes_t, weight_t, wg, wu, wd)


def shards(
    query_nope,
    query_rope,
    latent,
    key_rope,
    resid,
    latent_gain,
    key_up,
    value_up,
    out_proj,
    norm_gain,
    expert_gate,
    expert_up,
    expert_down,
    routes,
    route_weight,
):
    tokens = latent.shape[1]
    positions = lax.axis_index("sp") * tokens + jnp.arange(tokens, dtype=jnp.int32)
    half_width = key_rope.shape[-1] // 2
    frequency = rope_base ** (-jnp.arange(half_width, dtype=jnp.float32) / half_width)
    angles = frequency[:, None] * positions.astype(jnp.float32)[None, :]
    return layer(
        query_nope[0], query_rope[0].transpose(1, 2, 0), latent[0], latent_gain[None],
        key_rope[0].T, jnp.cos(angles), jnp.sin(angles), key_up, value_up, out_proj, resid[0], norm_gain[None],
        routes[0].T, route_weight[0].T, expert_gate[0], expert_up[0], expert_down[0],
    ).astype(jnp.bfloat16)[None]


def solution(mesh):
    return jax.shard_map(
        shards,
        mesh=mesh,
        in_specs=(
            P("dp", "sp", None, None),
            P("dp", "sp", None, None),
            P("dp", "sp", None),
            P("dp", "sp", None),
            P("dp", "sp", None),
            P(),
            P(None, "sp"),
            P(None, "sp"),
            P("sp", "dp"),
            P(),
            P("sp", None, None),
            P("sp", None, None),
            P("sp", None, None),
            P("dp", "sp", None),
            P("dp", "sp", None),
        ),
        out_specs=P("dp", "sp", None),
        check_vma=False,
    )
```
